256 devices in a mesh: sp: 64 (over z, x, core), tp: 4 (over y).
Axes of the slice: x: 4, y: 4, z: 8, core: 2. Of those that a mesh axis runs over, the one named last changes fastest.
Arguments:
- residual: bfloat16 [16384, 2048], P(('sp', 'tp')), may hold values from -6 to 6
- queries: bfloat16 [16384, 1024], P('sp', 'tp'), may hold values from -8 to 8
- key_pairs: bfloat16 [16384, 512], P('sp', 'tp'), may hold values from -8 to 8
- values: bfloat16 [16384, 512], P('sp', 'tp'), may hold values from -6 to 6
- lambdas: float32 [8], P('tp'), may hold values from 0.3 to 0.8
- head_gain: float32 [128], replicated, may hold values from 0.1 to 1.9
- out_weight: bfloat16 [1024, 2048], replicated, may hold values from -0.1875 to 0.1875
- mixer_gain: float32 [2048], replicated, may hold values from 0.1 to 1.9
- before_gain: float32 [2048], replicated, may hold values from 0.1 to 1.9
- after_gain: float32 [2048], replicated, may hold values from 0.1 to 1.9
- gate_weight: bfloat16 [2048, 5632], P('sp', 'tp'), may hold values from -0.125 to 0.125
- up_weight: bfloat16 [2048, 5632], P('sp', 'tp'), may hold values from -0.125 to 0.125
- down_weight: bfloat16 [5632, 2048], P('tp', 'sp'), may hold values from -0.078125 to 0.078125
Outputs:
- updated: bfloat16 [16384, 2048], P(('sp', 'tp'))
The draws below stay inside these ranges and needn't reach their ends.
All inputs are finite; a program needn't handle non-finite values.
Results may differ from the reference program's by a relative error of at most 0.014.
Values may be sent and summed in bfloat16 or wider, within the bound.
No kernel may reach another device: no remote copies, remote signals or barrier semaphores. Data moves between devices by JAX's collectives and lax.ppermute only.
A program may use at most 128 MiB of HBM per device.

```python
import math
import jax
import jax.numpy as jnp
from jax import lax

D = 2048
FF = 5632
HEADS = 8
KV_HEADS = 4
HEAD_DIM = 64
TOKENS = 16384
N_TP = 4


def drawn_pair(key):
    query_key, key_key = jax.random.split(key, 2)
    query_draw = jnp.clip(1.3 * jax.random.normal(query_key, (TOKENS, HEADS, 2, HEAD_DIM), jnp.float32), -7.5, 7.5)
    key_draw = jnp.clip(1.3 * jax.random.normal(key_key, (TOKENS, KV_HEADS, 2, HEAD_DIM), jnp.float32), -7.5, 7.5)
    return (query_draw, key_draw)


def draw_queries(key, part):
    query_draw = drawn_pair(jax.random.fold_in(key, 17))[0]
    return query_draw.reshape(TOKENS, HEADS * 2 * HEAD_DIM).astype(jnp.bfloat16)


def draw_key_pairs(key, part):
    key_draw = drawn_pair(jax.random.fold_in(key, 17))[1]
    return key_draw.reshape(TOKENS, KV_HEADS * 2 * HEAD_DIM).astype(jnp.bfloat16)


def level_of(rng, dims, cuts, low, largest):
    loudness, own = 1.0, jax.random.fold_in(rng, 6)
    for axis_at, shards_of in cuts:
        draws = jnp.exp(jax.random.uniform(jax.random.fold_in(own, axis_at), (shards_of,), jnp.float32, low / len(cuts), largest / len(cuts)))
        loudness = loudness * jnp.repeat(draws, dims[axis_at] // shards_of).reshape([-1 if axis == axis_at else 1 for axis in range(len(dims))])
    return loudness


def normal_values(own_key, shape, scale, bound, shards=(), held_as=jnp.bfloat16):
    level = level_of(own_key, shape, shards, -0.22, 0.18) if shards else 1.0
    values = jax.random.normal(own_key, shape, jnp.float32) * scale * level
    return jnp.minimum(jnp.maximum(values, -bound), bound).astype(held_as)


def setup_inputs(seed: int = 0) -> dict:
    arg_keys = jax.random.split(jax.random.key(seed), 14)
    residual = normal_values(arg_keys[0], (TOKENS, D), 1.0, 6.0, ((0, 256),))
    queries = draw_queries(jax.random.fold_in(arg_keys[13], 71), 0)
    key_pairs = draw_key_pairs(jax.random.fold_in(arg_keys[13], 71), 0)
    values = normal_values(arg_keys[3], (TOKENS, KV_HEADS * 2 * HEAD_DIM), 1.0, 6.0, ((0, 64), (1, 4)))
    lambdas = jnp.clip(0.3 + 0.5 * jax.random.uniform(arg_keys[4], (HEADS,), jnp.float32) ** level_of(arg_keys[4], (HEADS,), ((0, 4),), -0.2, 0.2), 0.3, 0.8)
    head_gain = jnp.clip(1.0 + 0.18 * jax.random.normal(arg_keys[5], (2 * HEAD_DIM,), jnp.float32), 0.1, 1.9)
    out_weight = normal_values(arg_keys[6], (HEADS * 2 * HEAD_DIM, D), (HEADS * 2 * HEAD_DIM) ** -0.5, 0.1875)
    mixer_gain = jnp.clip(1.0 + 0.18 * jax.random.normal(arg_keys[7], (D,), jnp.float32), 0.1, 1.9)
    before_gain = jnp.clip(1.0 + 0.18 * jax.random.normal(arg_keys[8], (D,), jnp.float32), 0.1, 1.9)
    after_gain = jnp.clip(1.0 + 0.18 * jax.random.normal(arg_keys[9], (D,), jnp.float32), 0.1, 1.9)
    gate_weight = normal_values(arg_keys[10], (D, FF), D ** -0.5, 0.125, ((0, 64), (1, 4)))
    up_weight = normal_values(arg_keys[11], (D, FF), D ** -0.5, 0.125, ((0, 64), (1, 4)))
    down_weight = normal_values(arg_keys[12], (FF, D), FF ** -0.5, 0.078125, ((0, 4), (1, 64)))
    return {"residual": residual, "queries": queries, "key_pairs": key_pairs, "values": values, "lambdas": lambdas, "head_gain": head_gain, "out_weight": out_weight, "mixer_gain": mixer_gain, "before_gain": before_gain, "after_gain": after_gain, "gate_weight": gate_weight, "up_weight": up_weight, "down_weight": down_weight}


def row_norm(values_in, gain, epsilon):
    mean_square = lax.optimization_barrier(jnp.mean(values_in * values_in, axis=-1, keepdims=True))
    return values_in * lax.rsqrt(mean_square + epsilon) * gain

def reference(residual, queries, key_pairs, values, lambdas, head_gain, out_weight, mixer_gain, before_gain, after_gain, gate_weight, up_weight, down_weight):
    group = HEADS // KV_HEADS
    scale = 1.0 / math.sqrt(HEAD_DIM)
    width = 2 * HEAD_DIM
    query_heads = jnp.transpose(queries.reshape(TOKENS, HEADS, 2, HEAD_DIM), (1, 2, 0, 3))
    key_heads = jnp.transpose(key_pairs.reshape(TOKENS, KV_HEADS, 2, HEAD_DIM), (1, 2, 0, 3))
    value_heads = jnp.transpose(values.reshape(TOKENS, KV_HEADS, width), (1, 0, 2))
    height = math.gcd(TOKENS, 512)
    blocks = TOKENS // height

    def one_block(index):
        head = index // blocks
        first = index % blocks * height
        shared = head // group
        zero = jnp.zeros((), jnp.int32)
        query_block = lax.dynamic_slice(query_heads, (head, zero, first, zero), (1, 2, height, HEAD_DIM))[0]
        key_block = lax.dynamic_index_in_dim(key_heads, shared, 0, keepdims=False)
        value_block = lax.dynamic_index_in_dim(value_heads, shared, 0, keepdims=False)
        second_weight = lax.dynamic_index_in_dim(lambdas, head, 0, keepdims=False)
        results = []
        for which in range(2):
            score = jnp.dot(query_block[which], key_block[which].T, preferred_element_type=jnp.float32) * scale
            top = lax.optimization_barrier(jnp.max(score, axis=1, keepdims=True))
            expo = jnp.exp(score - top)
            total = lax.optimization_barrier(jnp.sum(expo, axis=1, keepdims=True))
            numer = jnp.dot(expo.astype(jnp.bfloat16), value_block, preferred_element_type=jnp.float32)
            results.append(numer / total)
        attended = results[0] - second_weight * results[1]
        return row_norm(attended, head_gain, 1e-05).astype(jnp.bfloat16)
    normed = lax.map(one_block, jnp.arange(HEADS * blocks, dtype=jnp.int32))
    head_out = jnp.transpose(normed.reshape(HEADS, TOKENS, width), (1, 0, 2)).reshape(TOKENS, HEADS * width)
    mixed = jnp.dot(head_out, out_weight, preferred_element_type=jnp.float32).astype(jnp.bfloat16)
    stream = residual.astype(jnp.float32) + row_norm(mixed.astype(jnp.float32), mixer_gain, 1e-06)
    normed_in = row_norm(stream, before_gain, 1e-06).astype(jnp.bfloat16)
    gate = jnp.dot(normed_in, gate_weight, preferred_element_type=jnp.float32)
    up = jnp.dot(normed_in, up_weight, preferred_element_type=jnp.float32)
    hidden = (jax.nn.silu(gate) * up).astype(jnp.bfloat16)
    group_width = FF // N_TP
    channel = jnp.zeros((TOKENS, D), jnp.float32)
    for member in range(N_TP):
        lower = member * group_width
        upper = lower + group_width
        term = jnp.dot(hidden[:, lower:upper], down_weight[lower:upper], preferred_element_type=jnp.float32).astype(jnp.bfloat16)
        channel = channel + lax.optimization_barrier(term).astype(jnp.float32)
    channel = channel.astype(jnp.bfloat16)
    updated = stream + 0.5 * row_norm(channel.astype(jnp.float32), after_gain, 1e-06)
    return updated.astype(jnp.bfloat16)
```

```python
import functools
import math

import jax
import jax.numpy as jnp
from jax import lax
from jax.experimental import pallas as pl
from jax.experimental.pallas import tpu as pltpu
from jax.sharding import Mesh
from jax.sharding import PartitionSpec as P

HEAD_DIM = 64
WIDTH = 2 * HEAD_DIM
Z, X, C, T = "sp_0", "sp_1", "sp_2", "tp"
SP = (Z, X, C)
SP_TP = (Z, X, C, T)
F32, BF16 = jnp.float32, jnp.bfloat16
LOG2E = 1.4426950408889634
VMEM = pl.BlockSpec(memory_space=pltpu.VMEM)
SMEM = pl.BlockSpec(memory_space=pltpu.SMEM)
STATE = WIDTH + 8
COLS = 256


def shifted(array, axis, by):
    count = lax.axis_size(axis)
    return lax.ppermute(array, axis, [((i + by) % count, i) for i in range(count)])


def attend_kernel(first, pieces, tiles, *refs):
    queries = refs[:2]
    kvs = refs[2 : 2 + pieces]
    refs = refs[2 + pieces :]
    ins, outs = (None, refs[:2]) if first else (refs[:2], refs[2:4])
    lane = lax.broadcasted_iota(jnp.int32, (COLS, WIDTH), 1)
    factor = LOG2E / math.sqrt(HEAD_DIM)
    for kv_at, kv in enumerate(kvs):
        keys = kv[:, :WIDTH]
        values_t = kv[:, WIDTH:].T
        for half in range(2):
            for which in range(2):
                for head in range(2):
                    at = pl.ds((which * 2 + head) * COLS, COLS)
                    query = queries[half][:, head * WIDTH : (head + 1) * WIDTH]
                    query = jnp.where((lane < HEAD_DIM) == (which == 0), query, jnp.zeros_like(query))
                    score = lax.dot_general(
                        keys, query, (((1,), (1,)), ((), ())), preferred_element_type=F32
                    )
                    top = jnp.max(score, axis=0, keepdims=True) * factor
                    src = None if first and kv_at == 0 else (ins if kv_at == 0 else outs)
                    if src is not None:
                        old_top = src[half][WIDTH : WIDTH + 1, at]
                        top = jnp.maximum(top, old_top)
                        shrink = jnp.exp2(old_top - top)
                    expo = jnp.exp2(score * factor - top)
                    total = jnp.sum(expo, axis=0, keepdims=True)
                    numer = lax.dot_general(
                        values_t, expo.astype(BF16), (((1,), (0,)), ((), ())), preferred_element_type=F32
                    )
                    if src is not None:
                        total = total + src[half][WIDTH + 1 : WIDTH + 2, at] * shrink
                        numer = numer + src[half][:WIDTH, at] * shrink
                    outs[half][:WIDTH, at] = numer
                    outs[half][WIDTH : WIDTH + 1, at] = top
                    outs[half][WIDTH + 1 : WIDTH + 2, at] = total


def attend(state, queries, kvs):
    first = state is None
    keys = sum(kv.shape[0] for kv in kvs)
    shape = jax.ShapeDtypeStruct((STATE, 4 * COLS), F32)
    operands = (*queries, *kvs, *(() if first else state))
    return pl.pallas_call(
        functools.partial(attend_kernel, first, len(kvs), 8),
        out_shape=(shape, shape),
        in_specs=[VMEM] * len(operands),
        out_specs=(VMEM, VMEM),
        input_output_aliases={} if first else {2 + len(kvs): 0, 3 + len(kvs): 1},
        compiler_params=pltpu.CompilerParams(vmem_limit_bytes=40 << 20),
        cost_estimate=pl.CostEstimate(
            flops=2 * 2048 * keys * 256 * 2, bytes_accessed=keys * 512 + (2 << 20), transcendentals=2048 * keys
        ),
        name="attend",
    )(*operands)


def merge_kernel(lambdas, mine, theirs, gain, out):
    for head in range(2):
        maps = []
        for which in range(2):
            at = pl.ds((which * 2 + head) * COLS, COLS)
            top_a, top_b = mine[WIDTH : WIDTH + 1, at], theirs[WIDTH : WIDTH + 1, at]
            top = jnp.maximum(top_a, top_b)
            weight_a, weight_b = jnp.exp2(top_a - top), jnp.exp2(top_b - top)
            total = mine[WIDTH + 1 : WIDTH + 2, at] * weight_a + theirs[WIDTH + 1 : WIDTH + 2, at] * weight_b
            maps.append((mine[:WIDTH, at] * weight_a + theirs[:WIDTH, at] * weight_b) / total)
        attended = maps[0] - lambdas[head] * maps[1]
        mean_square = jnp.mean(attended * attended, axis=0, keepdims=True)
        normed = attended * lax.rsqrt(mean_square + 1e-05) * gain[...]
        out[:, head * WIDTH : (head + 1) * WIDTH] = normed.T.astype(BF16)


def merge(lambdas, mine, theirs, gain):
    return pl.pallas_call(
        merge_kernel,
        out_shape=jax.ShapeDtypeStruct((COLS, 2 * WIDTH), BF16),
        in_specs=[SMEM, VMEM, VMEM, VMEM],
        out_specs=VMEM,
        cost_estimate=pl.CostEstimate(flops=1 << 22, bytes_accessed=1 << 21, transcendentals=0),
        name="merge",
    )(lambdas, mine, theirs, gain.reshape(WIDTH, 1))


def row_norm(rows, gain, epsilon):
    mean_square = jnp.mean(rows * rows, axis=-1, keepdims=True)
    return rows * lax.rsqrt(mean_square + epsilon) * gain


def project_kernel(me, h0, h1, h2, h3, r0, r1, r2, r3, weight, mixer_gain, before_gain, normed_out, stream_out, mixed):
    group = h0.shape[1]
    quarter = r0.shape[0]
    for j, heads in enumerate((h0, h1, h2, h3)):
        rows = pl.ds(pl.multiple_of(lax.rem(me[0] + j, 4) * group, group), group)
        term = jnp.dot(heads[...], weight[rows, :], preferred_element_type=F32)
        if j == 0:
            mixed[...] = term
        else:
            mixed[...] += term
    for k, residual in enumerate((r0, r1, r2, r3)):
        rows = pl.ds(pl.multiple_of(lax.rem(me[0] + k, 4) * quarter, quarter), quarter)
        block = mixed[rows, :].astype(BF16).astype(F32)
        stream = residual[...].astype(F32) + row_norm(block, mixer_gain[...], 1e-06)
        if k == 0:
            stream_out[...] = stream
        normed_out[k * quarter : (k + 1) * quarter, :] = row_norm(stream, before_gain[...], 1e-06).astype(BF16)


def project(me, heads, residuals, weight, mixer_gain, before_gain):
    tokens, width = heads[0].shape[0], weight.shape[1]
    return pl.pallas_call(
        project_kernel,
        out_shape=(
            jax.ShapeDtypeStruct((tokens, width), BF16),
            jax.ShapeDtypeStruct((tokens // 4, width), F32),
        ),
        in_specs=[SMEM] + [VMEM] * 11,
        out_specs=(VMEM, VMEM),
        scratch_shapes=[pltpu.VMEM((tokens, width), F32)],
        compiler_params=pltpu.CompilerParams(vmem_limit_bytes=40 << 20),
        cost_estimate=pl.CostEstimate(
            flops=2 * tokens * width * weight.shape[0], bytes_accessed=8 << 20, transcendentals=0
        ),
        name="project",
    )(me, *heads, *residuals, weight, mixer_gain.reshape(1, width), before_gain.reshape(1, width))


def mix_kernel(gate_steps, x, gate_up, down, o0, o1, o2, o3, hidden):
    step = pl.program_id(0)

    @pl.when(step < gate_steps)
    def _():
        both = jnp.dot(x[...], gate_up[...], preferred_element_type=F32)
        gate, up = both[:, :128], both[:, 128:]
        hidden[:, pl.ds(pl.multiple_of(step * 128, 128), 128)] = (gate / (1.0 + jnp.exp(-gate)) * up).astype(BF16)

    @pl.when(step >= gate_steps)
    def _():
        part = lax.dot_general(
            hidden[...], down[...], (((1,), (1,)), ((), ())), preferred_element_type=F32
        ).astype(BF16)
        for k, out in enumerate((o0, o1, o2, o3)):
            rows = out.shape[0]
            out[...] = part[k * rows : (k + 1) * rows]


def mix(x, weights, units):
    tokens, width = x.shape
    gate_steps = units // 128
    wide = 512
    down_steps = width // wide
    quarter = tokens // 4
    shape = jax.ShapeDtypeStruct((quarter, width), BF16)
    late = lambda i: jnp.maximum(i - gate_steps, 0)
    return pl.pallas_call(
        functools.partial(mix_kernel, gate_steps),
        grid=(gate_steps + down_steps,),
        out_shape=(shape,) * 4,
        in_specs=[
            pl.BlockSpec((tokens, width), lambda i: (0, 0)),
            pl.BlockSpec((width, 256), lambda i: (0, jnp.minimum(i, gate_steps - 1))),
            pl.BlockSpec((wide, units), lambda i: (late(i), 2)),
        ],
        out_specs=(pl.BlockSpec((quarter, wide), lambda i: (0, late(i))),) * 4,
        scratch_shapes=[pltpu.VMEM((tokens, units), BF16)],
        compiler_params=pltpu.CompilerParams(vmem_limit_bytes=40 << 20),
        cost_estimate=pl.CostEstimate(
            flops=6 * tokens * width * units, bytes_accessed=6 * width * units, transcendentals=0
        ),
        name="mix",
    )(x, weights, weights)


def on_device(
    residual,
    queries,
    key_pairs,
    values,
    lambdas,
    head_gain,
    out_weight,
    mixer_gain,
    before_gain,
    after_gain,
    gate_weight,
    up_weight,
    down_weight,
):
    me = lax.axis_index(T).reshape(1)
    units = gate_weight.shape[1]
    rows = gate_weight.shape[0]
    gate_up = jnp.stack(
        (gate_weight.reshape(rows, units // 128, 128), up_weight.reshape(rows, units // 128, 128)), axis=2
    ).reshape(rows, 2 * units)
    packed = jnp.concatenate((gate_up, down_weight.T), axis=1)
    weights = lax.all_gather(packed, SP, axis=0, tiled=True)

    kv = jnp.concatenate((key_pairs, values), axis=1)
    other_queries = shifted(queries, C, 1)
    q = (queries, other_queries)
    row = jnp.concatenate((kv, shifted(kv, X, 1), shifted(kv, X, -1), shifted(kv, X, 2)), axis=0)
    ring = lax.axis_size(Z)
    state = None
    above = below = row
    state = attend(state, q, (row,))
    for step in range(1, ring // 2 + 1):
        if step < ring // 2:
            above, below = shifted(above, Z, 1), shifted(below, Z, -1)
            pieces = (above, below)
        else:
            half = row.shape[0] // 2
            pieces = (shifted(above[:half], Z, 1), shifted(below[half:], Z, -1))
        state = attend(state, q, pieces)
    mine, theirs = state
    theirs = shifted(theirs, C, 1)
    head_out = merge(lambdas, mine, theirs, head_gain)

    residuals = [residual] + [shifted(residual, T, k) for k in (1, 2, 3)]
    heads = [head_out] + [shifted(head_out, T, k) for k in (1, 2, 3)]
    normed_in, stream = project(me, heads, residuals, out_weight, mixer_gain, before_gain)
    parts = mix(normed_in, weights, units)
    arrived = [parts[0]] + [shifted(parts[k], T, -k) for k in (1, 2, 3)]
    channel = sum(part.astype(F32) for part in arrived).astype(BF16)
    updated = stream + 0.5 * row_norm(channel.astype(F32), after_gain, 1e-06)
    return updated.astype(BF16)


def solution(mesh):
    finer = Mesh(mesh.devices.reshape(8, 4, 2, mesh.shape[T]), SP_TP)
    in_specs = (
        P(SP_TP, None),
        P(SP, T),
        P(SP, T),
        P(SP, T),
        P(T),
        P(),
        P(),
        P(),
        P(),
        P(),
        P(SP, T),
        P(SP, T),
        P(T, SP),
    )
    return jax.shard_map(
        on_device, mesh=finer, in_specs=in_specs, out_specs=P(SP_TP, None), check_vma=False
    )
```

```python
import functools
import math

import jax
import jax.numpy as jnp
from jax import lax
from jax.experimental import pallas as pl
from jax.experimental.pallas import tpu as pltpu
from jax.sharding import Mesh
from jax.sharding import PartitionSpec as P

HEAD_DIM = 64
WIDTH = 2 * HEAD_DIM
Z, X, C, T = "sp_0", "sp_1", "sp_2", "tp"
SP = (Z, X, C)
SP_TP = (Z, X, C, T)
F32, BF16 = jnp.float32, jnp.bfloat16
LOG2E = 1.4426950408889634
VMEM = pl.BlockSpec(memory_space=pltpu.VMEM)
SMEM = pl.BlockSpec(memory_space=pltpu.SMEM)
STATE = WIDTH + 8
COLS = 256
PIECE = 256
TALL = WIDTH + 16
FACTOR = LOG2E / math.sqrt(HEAD_DIM)
LIMIT = 2.0**80


def shifted(array, axis, by):
    count = lax.axis_size(axis)
    return lax.ppermute(array, axis, [((i + by) % count, i) for i in range(count)])


def attend_kernel(first, count, groups, *refs):
    if first:
        queries, kvs, refs = refs[:2], refs[2 : 2 + count], refs[2 + count :]
        ins, (out_a, out_b, tables, keys2, values1) = None, refs
        old_tables = tables
    else:
        kvs, ins, old_tables, refs = refs[:count], refs[count : count + 2], refs[count + 2], refs[count + 3 :]
        out_a, out_b, tables, keys2, values1 = refs
    outs = (out_a, out_b)
    length = values1.shape[1]
    lane = lax.broadcasted_iota(jnp.int32, (1, WIDTH), 1)
    values1[WIDTH:, :] = jnp.ones((TALL - WIDTH, length), BF16)
    at = 0
    for kv in kvs:
        span = pl.ds(at, kv.shape[0])
        keys = kv[:, :WIDTH]
        for which in range(2):
            keys2[which, span, :WIDTH] = keys
            keys2[which, span, WIDTH:] = jnp.where((lane < HEAD_DIM) == (which == 0), keys, jnp.ones_like(keys))
        values1[:WIDTH, span] = kv[:, WIDTH:].T
        at += kv.shape[0]
    row = lax.broadcasted_iota(jnp.int32, (WIDTH, COLS), 0)
    if first:

        def one_table(group, carry):
            rows = pl.ds(pl.multiple_of(group * COLS, COLS), COLS)
            for half in range(2):
                for head in range(2):
                    query = queries[half][rows, head * WIDTH : (head + 1) * WIDTH].astype(F32).T * FACTOR
                    high = query.astype(BF16).astype(F32)
                    low = query - high
                    for which in range(2):
                        own = (row < HEAD_DIM) == (which == 0)
                        tile = group * 4 + which * 2 + head
                        table = tables.at[half * 4 * groups + tile]
                        lower = jnp.where(own, low, 0.0)
                        table[:WIDTH, :] = jnp.where(own, high, 0.0).astype(BF16)
                        table[WIDTH:, :] = lower.astype(BF16)
                        score = jnp.dot(keys2[which, :COLS, :], table[...], preferred_element_type=F32)
                        top = jnp.max(score, axis=0, keepdims=True).astype(BF16).astype(F32)
                        spot = HEAD_DIM if which == 0 else 0
                        table[WIDTH:, :] = jnp.where(row == spot, -top, lower).astype(BF16)
                        outs[half][tile, WIDTH:, :] = jnp.broadcast_to(top, (8, COLS))
            return carry

        lax.fori_loop(0, groups, one_table, 0)
    line = lax.broadcasted_iota(jnp.int32, (8, COLS), 0)
    piece = length // pl.cdiv(length, PIECE)

    def one_group(group, largest):
        for half in range(2):
            for kind in range(4):
                tile = group * 4 + kind
                table = old_tables[half * 4 * groups + tile]
                both = None
                for start in range(0, length, piece):
                    score = jnp.dot(keys2[kind // 2, start : start + piece, :], table, preferred_element_type=F32)
                    expo = jnp.exp2(score).astype(BF16)
                    term = jnp.dot(values1[:, start : start + piece], expo, preferred_element_type=F32)
                    both = term if both is None else both + term
                numer, total = both[:WIDTH], both[WIDTH:STATE]
                if first:
                    top = outs[half][tile, WIDTH : WIDTH + 1, :]
                else:
                    top = ins[half][tile, WIDTH : WIDTH + 1, :]
                    numer = numer + ins[half][tile, :WIDTH, :]
                    total = total + ins[half][tile, WIDTH + 1 : WIDTH + 2, :]
                outs[half][tile, :WIDTH, :] = numer
                outs[half][tile, WIDTH:, :] = jnp.where(line == 0, jnp.broadcast_to(top, (8, COLS)), total)
                largest = jnp.maximum(largest, jnp.where(total[0:1] < LIMIT, 0.0, 1.0))
        return largest

    largest = lax.fori_loop(0, groups, one_group, jnp.zeros((1, COLS), F32))

    @pl.when(jnp.max(largest) > 0.0)
    def _():
        def one_tile(tile, carry):
            which = lax.rem(tile, 4) // 2
            for half in range(2):
                table = tables.at[half * 4 * groups + tile]

                def score_of(i):
                    rows = pl.ds(pl.multiple_of(i * COLS, COLS), COLS)
                    return jnp.dot(keys2[which, rows, :], table[...], preferred_element_type=F32), rows

                def find_top(i, top):
                    return jnp.maximum(top, jnp.max(score_of(i)[0], axis=0, keepdims=True))

                above = lax.fori_loop(0, length // COLS, find_top, jnp.zeros((1, COLS), F32))
                spot = jnp.where(which == 0, HEAD_DIM, 0)
                old_top = outs[half][tile, WIDTH : WIDTH + 1, :] if first else ins[half][tile, WIDTH : WIDTH + 1, :]
                top = (old_top + above).astype(BF16).astype(F32)
                raised = top - old_top

                def add(i, both):
                    score, rows = score_of(i)
                    expo = jnp.exp2(score - raised).astype(BF16)
                    cols = pl.ds(pl.multiple_of(i * COLS, COLS), COLS)
                    return both + jnp.dot(values1[:, cols], expo, preferred_element_type=F32)

                both = lax.fori_loop(0, length // COLS, add, jnp.zeros((TALL, COLS), F32))
                numer, total = both[:WIDTH], both[WIDTH:STATE]
                if not first:
                    shrink = jnp.exp2(-raised)
                    numer = numer + ins[half][tile, :WIDTH, :] * shrink
                    total = total + ins[half][tile, WIDTH + 1 : WIDTH + 2, :] * shrink
                outs[half][tile, :WIDTH, :] = numer
                outs[half][tile, WIDTH:, :] = jnp.where(line == 0, jnp.broadcast_to(top, (8, COLS)), total)
                lower = table[WIDTH:, :].astype(F32)
                table[WIDTH:, :] = jnp.where(row == spot, -top, lower).astype(BF16)
            return carry

        lax.fori_loop(0, 4 * groups, one_tile, 0)


def attend(carried, queries, kvs):
    first = carried is None
    keys = sum(kv.shape[0] for kv in kvs)
    groups = queries[0].shape[0] // COLS
    state = jax.ShapeDtypeStruct((4 * groups, STATE, COLS), F32)
    tables = jax.ShapeDtypeStruct((8 * groups, 2 * WIDTH, COLS), BF16)
    operands = (*queries, *kvs) if first else (*kvs, *carried)
    return pl.pallas_call(
        functools.partial(attend_kernel, first, len(kvs), groups),
        out_shape=(state, state, tables),
        in_specs=[VMEM] * len(operands),
        out_specs=(VMEM,) * 3,
        scratch_shapes=[pltpu.VMEM((2, keys, 2 * WIDTH), BF16), pltpu.VMEM((TALL, keys), BF16)],
        input_output_aliases={} if first else {len(kvs) + 2: 2},
        compiler_params=pltpu.CompilerParams(vmem_limit_bytes=40 << 20),
        cost_estimate=pl.CostEstimate(
            flops=2 * 2048 * groups * keys * 256 * 2,
            bytes_accessed=keys * 512 + (2 << 20),
            transcendentals=2048 * groups * keys,
        ),
        name="attend",
    )(*operands)


def halves_kernel(mine, theirs, own, *sent):
    line = lax.broadcasted_iota(jnp.int32, (8, COLS), 0)

    def joined(tile):
        a, b = mine.at[tile], theirs.at[tile]
        top_a, top_b = a[WIDTH : WIDTH + 1, :], b[WIDTH : WIDTH + 1, :]
        top = jnp.maximum(top_a, top_b)
        weight_a, weight_b = jnp.exp2(top_a - top), jnp.exp2(top_b - top)
        total = a[WIDTH + 1 : WIDTH + 2, :] * weight_a + b[WIDTH + 1 : WIDTH + 2, :] * weight_b
        return (a[:WIDTH, :] * weight_a + b[:WIDTH, :] * weight_b) / total, top + jnp.log2(total)

    for kind in range(4):
        outcome, level = joined(kind)
        own[kind, :WIDTH, :] = outcome
        own[kind, WIDTH:, :] = jnp.broadcast_to(level, (8, COLS))
        for group, out in enumerate(sent):
            outcome, level = joined(4 * (group + 1) + kind)
            out[kind, :WIDTH, :] = outcome.astype(BF16)
            high = level.astype(BF16).astype(F32)
            middle = (level - high).astype(BF16).astype(F32)
            low = level - high - middle
            parts = jnp.where(line == 0, high, jnp.where(line == 1, middle, low))
            out[kind, WIDTH:, :] = jnp.concatenate((parts, jnp.zeros_like(parts)), axis=0).astype(BF16)


def join_halves(mine, theirs):
    groups = mine.shape[0] // 4
    sent = jax.ShapeDtypeStruct((4, TALL, COLS), BF16)
    return pl.pallas_call(
        halves_kernel,
        out_shape=(jax.ShapeDtypeStruct((4, STATE, COLS), F32),) + (sent,) * (groups - 1),
        in_specs=[VMEM, VMEM],
        out_specs=(VMEM,) * groups,
        compiler_params=pltpu.CompilerParams(vmem_limit_bytes=40 << 20),
        cost_estimate=pl.CostEstimate(flops=1 << 24, bytes_accessed=1 << 22, transcendentals=0),
        name="join_halves",
    )(mine, theirs)


def merge_kernel(lambdas, own, *refs):
    *parts, gain, out = refs
    for head in range(2):
        maps = []
        for which in range(2):
            kind = which * 2 + head
            levels, outcomes = [own[kind, WIDTH : WIDTH + 1, :]], [own[kind, :WIDTH, :]]
            for part in parts:
                stats = part[kind, WIDTH:, :].astype(F32)
                levels.append(stats[0:1] + stats[1:2] + stats[2:3])
                outcomes.append(part[kind, :WIDTH, :].astype(F32))
            top = functools.reduce(jnp.maximum, levels)
            weights = [jnp.exp2(level - top) for level in levels]
            total = sum(weights)
            maps.append(sum(o * (w / total) for o, w in zip(outcomes, weights)))
        attended = maps[0] - lambdas[head] * maps[1]
        mean_square = jnp.mean(attended * attended, axis=0, keepdims=True)
        normed = attended * lax.rsqrt(mean_square + 1e-05)
        out[:, head * WIDTH : (head + 1) * WIDTH] = (normed.T * gain[...]).astype(BF16)


def merge(lambdas, own, parts, gain):
    return pl.pallas_call(
        merge_kernel,
        out_shape=jax.ShapeDtypeStruct((COLS, 2 * WIDTH), BF16),
        in_specs=[SMEM] + [VMEM] * (2 + len(parts)),
        out_specs=VMEM,
        cost_estimate=pl.CostEstimate(flops=1 << 22, bytes_accessed=1 << 21, transcendentals=0),
        name="merge",
    )(lambdas, own, *parts, gain.reshape(1, WIDTH))


def row_norm(rows, gain, epsilon):
    mean_square = jnp.mean(rows * rows, axis=-1, keepdims=True)
    return rows * lax.rsqrt(mean_square + epsilon) * gain


def project_kernel(me, h0, h1, h2, h3, r0, r1, r2, r3, weight, mixer_gain, before_gain, normed_out, stream_out, mixed):
    group = h0.shape[1]
    quarter = r0.shape[0]
    for j, heads in enumerate((h0, h1, h2, h3)):
        rows = pl.ds(pl.multiple_of(lax.rem(me[0] + j, 4) * group, group), group)
        term = jnp.dot(heads[...], weight[rows, :], preferred_element_type=F32)
        if j == 0:
            mixed[...] = term
        else:
            mixed[...] += term
    for k, residual in enumerate((r0, r1, r2, r3)):
        rows = pl.ds(pl.multiple_of(lax.rem(me[0] + k, 4) * quarter, quarter), quarter)
        block = mixed[rows, :].astype(BF16).astype(F32)
        stream = residual[...].astype(F32) + row_norm(block, mixer_gain[...], 1e-06)
        if k == 0:
            stream_out[...] = stream
        normed_out[k * quarter : (k + 1) * quarter, :] = row_norm(stream, before_gain[...], 1e-06).astype(BF16)


def project(me, heads, residuals, weight, mixer_gain, before_gain):
    tokens, width = heads[0].shape[0], weight.shape[1]
    return pl.pallas_call(
        project_kernel,
        out_shape=(
            jax.ShapeDtypeStruct((tokens, width), BF16),
            jax.ShapeDtypeStruct((tokens // 4, width), F32),
        ),
        in_specs=[SMEM] + [VMEM] * 11,
        out_specs=(VMEM, VMEM),
        scratch_shapes=[pltpu.VMEM((tokens, width), F32)],
        compiler_params=pltpu.CompilerParams(vmem_limit_bytes=40 << 20),
        cost_estimate=pl.CostEstimate(
            flops=2 * tokens * width * weight.shape[0], bytes_accessed=8 << 20, transcendentals=0
        ),
        name="project",
    )(me, *heads, *residuals, weight, mixer_gain.reshape(1, width), before_gain.reshape(1, width))


CHUNK = 256
AHEAD = 6


def mix_kernel(units, x, weights, o0, o1, o2, o3, held, hidden, sems):
    width = x.shape[1]
    tall = width // 4
    starts = range(0, units, CHUNK)
    copies = []
    for start in starts:
        cols = min(CHUNK, units - start)
        for j in range(2):
            at = pl.ds(j * units + start, cols)
            copies.append(pltpu.make_async_copy(weights.at[:, at], held.at[:, at], sems.at[len(copies)]))
    for i in range(4):
        rows, cols = pl.ds(i * tall, tall), pl.ds(2 * units, units)
        copies.append(pltpu.make_async_copy(weights.at[rows, cols], held.at[rows, cols], sems.at[len(copies)]))
    for copy in copies[:AHEAD]:
        copy.start()

    def wait(i):
        copies[i].wait()
        if i + AHEAD < len(copies):
            copies[i + AHEAD].start()

    for i, start in enumerate(starts):
        cols = min(CHUNK, units - start)
        wait(2 * i)
        wait(2 * i + 1)
        gate = jnp.dot(x[...], held[:, start : start + cols], preferred_element_type=F32)
        up = jnp.dot(x[...], held[:, units + start : units + start + cols], preferred_element_type=F32)
        hidden[:, start : start + cols] = (gate / (1.0 + jnp.exp(-gate)) * up).astype(BF16)
    for i in range(4):
        wait(2 * len(starts) + i)
        part = lax.dot_general(
            hidden[...],
            held[i * tall : (i + 1) * tall, 2 * units :],
            (((1,), (1,)), ((), ())),
            preferred_element_type=F32,
        ).astype(BF16)
        for k, out in enumerate((o0, o1, o2, o3)):
            rows = out.shape[0]
            out[:, i * tall : (i + 1) * tall] = part[k * rows : (k + 1) * rows]


def mix(x, weights, units):
    tokens, width = x.shape
    shape = jax.ShapeDtypeStruct((tokens // 4, width), BF16)
    return pl.pallas_call(
        functools.partial(mix_kernel, units),
        out_shape=(shape,) * 4,
        in_specs=[VMEM, pl.BlockSpec(memory_space=pl.ANY)],
        out_specs=(VMEM,) * 4,
        scratch_shapes=[
            pltpu.VMEM(weights.shape, BF16),
            pltpu.VMEM((tokens, units), BF16),
            pltpu.SemaphoreType.DMA((2 * pl.cdiv(units, CHUNK) + 4,)),
        ],
        compiler_params=pltpu.CompilerParams(vmem_limit_bytes=40 << 20),
        cost_estimate=pl.CostEstimate(
            flops=6 * tokens * width * units, bytes_accessed=6 * width * units, transcendentals=0
        ),
        name="mix",
    )(x, weights)


def on_device(
    residual,
    queries,
    key_pairs,
    values,
    lambdas,
    head_gain,
    out_weight,
    mixer_gain,
    before_gain,
    after_gain,
    gate_weight,
    up_weight,
    down_weight,
):
    me = lax.axis_index(T).reshape(1)
    units = gate_weight.shape[1]
    packed = jnp.concatenate((gate_weight, up_weight, down_weight.T), axis=1)
    weights = lax.all_gather(packed, SP, axis=0, tiled=True)

    kv = jnp.concatenate((key_pairs, values), axis=1)
    beside = [(i, i ^ 1) for i in range(lax.axis_size(X))]
    kv = jnp.concatenate((kv, lax.ppermute(kv, X, beside)), axis=0)
    own_queries = jnp.concatenate((queries, shifted(queries, X, 2)), axis=0)
    queries = (own_queries, shifted(own_queries, C, 1))
    residuals = [residual] + [shifted(residual, T, k) for k in (1, 2, 3)]
    kv, queries = lax.optimization_barrier((kv, queries))
    carried, pieces = None, (kv,)
    above = below = kv
    for step in range(1, lax.axis_size(Z) // 2):
        above, below = shifted(above, Z, 1), shifted(below, Z, -1)
        carried = attend(carried, queries, pieces)
        if step == 2:
            carried, residuals = lax.optimization_barrier((carried, residuals))
        carried, above, below = lax.optimization_barrier((carried, above, below))
        pieces = (above, below)
    half = kv.shape[0] // 2
    far = (shifted(above[:half], Z, 1), shifted(below[half:], Z, -1))
    carried = attend(carried, queries, pieces)
    mine, theirs, _ = attend(carried, queries, far)
    own, sent = join_halves(mine, shifted(theirs, C, 1))
    head_out = merge(lambdas, own, [shifted(sent, X, 2)], head_gain)

    heads = [head_out] + [shifted(head_out, T, k) for k in (1, 2, 3)]
    normed_in, stream = project(me, heads, residuals, out_weight, mixer_gain, before_gain)
    parts = mix(normed_in, weights, units)
    arrived = [parts[0]] + [shifted(parts[k], T, -k) for k in (1, 2, 3)]
    channel = sum(part.astype(F32) for part in arrived).astype(BF16)
    updated = stream + 0.5 * row_norm(channel.astype(F32), after_gain, 1e-06)
    return updated.astype(BF16)


def solution(mesh):
    finer = Mesh(mesh.devices.reshape(8, 4, 2, mesh.shape[T]), SP_TP)
    in_specs = (
        P(SP_TP, None),
        P(SP, T),
        P(SP, T),
        P(SP, T),
        P(T),
        P(),
        P(),
        P(),
        P(),
        P(),
        P(SP, T),
        P(SP, T),
        P(T, SP),
    )
    return jax.shard_map(
        on_device, mesh=finer, in_specs=in_specs, out_specs=P(SP_TP, None), check_vma=False
    )
```

```python
import functools
import math

import jax
import jax.numpy as jnp
from jax import lax
from jax.experimental import pallas as pl
from jax.experimental.pallas import tpu as pltpu
from jax.sharding import Mesh
from jax.sharding import PartitionSpec as P

HEAD_DIM = 64
WIDTH = 2 * HEAD_DIM
Z, X, C, T = "sp_0", "sp_1", "sp_2", "tp"
SP = (Z, X, C)
SP_TP = (Z, X, C, T)
F32, BF16 = jnp.float32, jnp.bfloat16
LOG2E = 1.4426950408889634
VMEM = pl.BlockSpec(memory_space=pltpu.VMEM)
SMEM = pl.BlockSpec(memory_space=pltpu.SMEM)
HBM = pl.BlockSpec(memory_space=pltpu.HBM)
STATE = WIDTH + 8
COLS = 256
PIECE = 256
TILES = 2
TALL = WIDTH + 16
FACTOR = LOG2E / math.sqrt(HEAD_DIM)
LIMIT = 2.0**80


def shifted(array, axis, by):
    count = lax.axis_size(axis)
    return lax.ppermute(array, axis, [((i + by) % count, i) for i in range(count)])


def attend_kernel(first, count, groups, *refs):
    if first:
        queries, kvs, refs = refs[:2], refs[2 : 2 + count], refs[2 + count :]
        ins, (out_a, out_b, tables, keys2, values1) = None, refs
    else:
        kvs, ins, tables, refs = refs[:count], refs[count : count + 2], refs[count + 2], refs[count + 3 :]
        out_a, out_b, keys2, values1 = refs
    outs = (out_a, out_b)
    length = values1.shape[1]
    lane = lax.broadcasted_iota(jnp.int32, (1, WIDTH), 1)
    values1[WIDTH:, :] = jnp.ones((TALL - WIDTH, length), BF16)
    at = 0
    for kv in kvs:
        span = pl.ds(at, kv.shape[0])
        keys = kv[:, :WIDTH]
        for which in range(2):
            keys2[which, span, :WIDTH] = keys
            keys2[which, span, WIDTH:] = jnp.where((lane < HEAD_DIM) == (which == 0), keys, jnp.ones_like(keys))
        values1[:WIDTH, span] = kv[:, WIDTH:].T
        at += kv.shape[0]
    row = lax.broadcasted_iota(jnp.int32, (WIDTH, COLS), 0)
    if first:

        def one_table(group, carry):
            rows = pl.ds(pl.multiple_of(group * COLS, COLS), COLS)
            for half in range(2):
                for head in range(2):
                    query = queries[half][rows, head * WIDTH : (head + 1) * WIDTH].astype(F32).T * FACTOR
                    high = query.astype(BF16).astype(F32)
                    low = query - high
                    for which in range(2):
                        own = (row < HEAD_DIM) == (which == 0)
                        tile = group * 4 + which * 2 + head
                        table = tables.at[half * 4 * groups + tile]
                        lower = jnp.where(own, low, 0.0)
                        table[:WIDTH, :] = jnp.where(own, high, 0.0).astype(BF16)
                        table[WIDTH:, :] = lower.astype(BF16)
                        score = jnp.dot(keys2[which, :COLS, :], table[...], preferred_element_type=F32)
                        top = jnp.max(score, axis=0, keepdims=True).astype(BF16).astype(F32)
                        spot = HEAD_DIM if which == 0 else 0
                        table[WIDTH:, :] = jnp.where(row == spot, -top, lower).astype(BF16)
                        outs[half][tile, WIDTH:, :] = jnp.broadcast_to(top, (8, COLS))
            return carry

        lax.fori_loop(0, groups, one_table, 0)
    line = lax.broadcasted_iota(jnp.int32, (8, COLS), 0)
    piece = length // pl.cdiv(length, PIECE)

    def stats_of(top, total, reference):
        top, reference = jnp.broadcast_to(top, (8, COLS)), jnp.broadcast_to(reference, (8, COLS))
        return jnp.where(line == 0, top, jnp.where(line == 2, reference, total))

    def one_tile(tile, largest):
        which = lax.rem(tile, 4) // 2
        for half in range(2):
            table = tables[half * 4 * groups + tile]
            both = None
            for start in range(0, length, piece):
                score = jnp.dot(keys2[which, start : start + piece, :], table, preferred_element_type=F32)
                expo = jnp.exp2(score).astype(BF16)
                term = jnp.dot(values1[:, start : start + piece], expo, preferred_element_type=F32)
                both = term if both is None else both + term
            numer, total = both[:WIDTH], both[WIDTH:STATE]
            stats = (outs if first else ins)[half][tile, WIDTH:, :]
            top, reference = stats[0:1], stats[2:3]
            if not first:
                numer = numer + ins[half][tile, :WIDTH, :]
                total = total + stats[1:2]
            outs[half][tile, :WIDTH, :] = numer
            outs[half][tile, WIDTH:, :] = stats_of(top, total, reference)
            fine = (total[0:1] < LIMIT) & (top == reference)
            largest = jnp.maximum(largest, jnp.where(fine, 0.0, 1.0))
        return largest

    def some_tiles(i, largest):
        for j in range(TILES):
            largest = one_tile(i * TILES + j, largest)
        return largest

    largest = lax.fori_loop(0, 4 * groups // TILES, some_tiles, jnp.zeros((1, COLS), F32))

    @pl.when(jnp.max(largest) > 0.0)
    def _():
        def redo_tile(tile, carry):
            which = lax.rem(tile, 4) // 2
            for half in range(2):
                table = tables.at[half * 4 * groups + tile]

                def score_of(i):
                    rows = pl.ds(pl.multiple_of(i * COLS, COLS), COLS)
                    return jnp.dot(keys2[which, rows, :], table[...], preferred_element_type=F32), rows

                def find_top(i, top):
                    return jnp.maximum(top, jnp.max(score_of(i)[0], axis=0, keepdims=True))

                above = lax.fori_loop(0, length // COLS, find_top, jnp.zeros((1, COLS), F32))
                stats = (outs if first else ins)[half][tile, WIDTH:, :]
                old_top, reference = stats[0:1], stats[2:3]
                top = jnp.maximum(old_top, reference + above)
                raised = top - reference

                def add(i, both):
                    score, rows = score_of(i)
                    expo = jnp.exp2(score - raised).astype(BF16)
                    cols = pl.ds(pl.multiple_of(i * COLS, COLS), COLS)
                    return both + jnp.dot(values1[:, cols], expo, preferred_element_type=F32)

                both = lax.fori_loop(0, length // COLS, add, jnp.zeros((TALL, COLS), F32))
                numer, total = both[:WIDTH], both[WIDTH:STATE]
                if not first:
                    shrink = jnp.exp2(old_top - top)
                    numer = numer + ins[half][tile, :WIDTH, :] * shrink
                    total = total + stats[1:2] * shrink
                outs[half][tile, :WIDTH, :] = numer
                outs[half][tile, WIDTH:, :] = stats_of(top, total, reference)
            return carry

        lax.fori_loop(0, 4 * groups, redo_tile, 0)


def attend(carried, queries, kvs):
    first = carried is None
    keys = sum(kv.shape[0] for kv in kvs)
    groups = queries[0].shape[0] // COLS
    state = jax.ShapeDtypeStruct((4 * groups, STATE, COLS), F32)
    tables = jax.ShapeDtypeStruct((8 * groups, 2 * WIDTH, COLS), BF16)
    operands = (*queries, *kvs) if first else (*kvs, *carried)
    results = (state, state, tables) if first else (state, state)
    done = pl.pallas_call(
        functools.partial(attend_kernel, first, len(kvs), groups),
        out_shape=results,
        in_specs=[VMEM] * len(operands),
        out_specs=(VMEM,) * len(results),
        scratch_shapes=[pltpu.VMEM((2, keys, 2 * WIDTH), BF16), pltpu.VMEM((TALL, keys), BF16)],
        compiler_params=pltpu.CompilerParams(vmem_limit_bytes=40 << 20),
        cost_estimate=pl.CostEstimate(
            flops=2 * 2048 * groups * keys * 256 * 2,
            bytes_accessed=keys * 512 + (2 << 20),
            transcendentals=2048 * groups * keys,
        ),
        name="attend",
    )(*operands)
    return done if first else (*done, carried[2])


def halves_kernel(mine, theirs, own, *sent):
    line = lax.broadcasted_iota(jnp.int32, (8, COLS), 0)

    def joined(tile):
        a, b = mine.at[tile], theirs.at[tile]
        top_a, top_b = a[WIDTH : WIDTH + 1, :], b[WIDTH : WIDTH + 1, :]
        top = jnp.maximum(top_a, top_b)
        weight_a, weight_b = jnp.exp2(top_a - top), jnp.exp2(top_b - top)
        total = a[WIDTH + 1 : WIDTH + 2, :] * weight_a + b[WIDTH + 1 : WIDTH + 2, :] * weight_b
        return (a[:WIDTH, :] * weight_a + b[:WIDTH, :] * weight_b) / total, top + jnp.log2(total)

    for kind in range(4):
        outcome, level = joined(kind)
        own[kind, :WIDTH, :] = outcome
        own[kind, WIDTH:, :] = jnp.broadcast_to(level, (8, COLS))
        for group, out in enumerate(sent):
            outcome, level = joined(4 * (group + 1) + kind)
            out[kind, :WIDTH, :] = outcome.astype(BF16)
            high = level.astype(BF16).astype(F32)
            middle = (level - high).astype(BF16).astype(F32)
            low = level - high - middle
            parts = jnp.where(line == 0, high, jnp.where(line == 1, middle, low))
            out[kind, WIDTH:, :] = jnp.concatenate((parts, jnp.zeros_like(parts)), axis=0).astype(BF16)


def join_halves(mine, theirs):
    groups = mine.shape[0] // 4
    sent = jax.ShapeDtypeStruct((4, TALL, COLS), BF16)
    return pl.pallas_call(
        halves_kernel,
        out_shape=(jax.ShapeDtypeStruct((4, STATE, COLS), F32),) + (sent,) * (groups - 1),
        in_specs=[VMEM, VMEM],
        out_specs=(VMEM,) * groups,
        compiler_params=pltpu.CompilerParams(vmem_limit_bytes=40 << 20),
        cost_estimate=pl.CostEstimate(flops=1 << 24, bytes_accessed=1 << 22, transcendentals=0),
        name="join_halves",
    )(mine, theirs)


def merge_kernel(lambdas, own, *refs):
    *parts, gain, out = refs
    for head in range(2):
        maps = []
        for which in range(2):
            kind = which * 2 + head
            levels, outcomes = [own[kind, WIDTH : WIDTH + 1, :]], [own[kind, :WIDTH, :]]
            for part in parts:
                stats = part[kind, WIDTH:, :].astype(F32)
                levels.append(stats[0:1] + stats[1:2] + stats[2:3])
                outcomes.append(part[kind, :WIDTH, :].astype(F32))
            top = functools.reduce(jnp.maximum, levels)
            weights = [jnp.exp2(level - top) for level in levels]
            total = sum(weights)
            maps.append(sum(o * (w / total) for o, w in zip(outcomes, weights)))
        attended = maps[0] - lambdas[head] * maps[1]
        mean_square = jnp.mean(attended * attended, axis=0, keepdims=True)
        normed = attended * lax.rsqrt(mean_square + 1e-05)
        out[:, head * WIDTH : (head + 1) * WIDTH] = (normed.T * gain[...]).astype(BF16)


def merge(lambdas, own, parts, gain):
    return pl.pallas_call(
        merge_kernel,
        out_shape=jax.ShapeDtypeStruct((COLS, 2 * WIDTH), BF16),
        in_specs=[SMEM] + [VMEM] * (2 + len(parts)),
        out_specs=VMEM,
        compiler_params=pltpu.CompilerParams(vmem_limit_bytes=8 << 20),
        cost_estimate=pl.CostEstimate(flops=1 << 22, bytes_accessed=1 << 21, transcendentals=0),
        name="merge",
    )(lambdas, own, *parts, gain.reshape(1, WIDTH))


def row_norm(rows, gain, epsilon):
    mean_square = jnp.mean(rows * rows, axis=-1, keepdims=True)
    return rows * lax.rsqrt(mean_square + epsilon) * gain


def project_kernel(me, h0, h1, h2, h3, r0, r1, r2, r3, weight, mixer_gain, before_gain, normed_out, stream_out, mixed, held, sems):
    group = h0.shape[1]
    quarter = r0.shape[0]
    copies = []
    for j in range(4):
        rows = pl.ds(pl.multiple_of(lax.rem(me[0] + j, 4) * group, group), group)
        copies.append(pltpu.make_async_copy(weight.at[rows, :], held.at[j], sems.at[j]))
        copies[j].start()
    for j, heads in enumerate((h0, h1, h2, h3)):
        copies[j].wait()
        term = jnp.dot(heads[...], held[j], preferred_element_type=F32)
        if j == 0:
            mixed[...] = term
        else:
            mixed[...] += term
    for k, residual in enumerate((r0, r1, r2, r3)):
        rows = pl.ds(pl.multiple_of(lax.rem(me[0] + k, 4) * quarter, quarter), quarter)
        block = mixed[rows, :].astype(BF16).astype(F32)
        stream = residual[...].astype(F32) + row_norm(block, mixer_gain[...], 1e-06)
        if k == 0:
            stream_out[...] = stream
        normed_out[k * quarter : (k + 1) * quarter, :] = row_norm(stream, before_gain[...], 1e-06).astype(BF16)


def project(me, heads, residuals, weight, mixer_gain, before_gain):
    tokens, width = heads[0].shape[0], weight.shape[1]
    return pl.pallas_call(
        project_kernel,
        out_shape=(
            jax.ShapeDtypeStruct((tokens, width), BF16),
            jax.ShapeDtypeStruct((tokens // 4, width), F32),
        ),
        in_specs=[SMEM] + [VMEM] * 8 + [HBM] + [VMEM] * 2,
        out_specs=(VMEM, VMEM),
        scratch_shapes=[
            pltpu.VMEM((tokens, width), F32),
            pltpu.VMEM((4, weight.shape[0] // 4, width), BF16),
            pltpu.SemaphoreType.DMA((4,)),
        ],
        compiler_params=pltpu.CompilerParams(vmem_limit_bytes=40 << 20),
        cost_estimate=pl.CostEstimate(
            flops=2 * tokens * width * weight.shape[0], bytes_accessed=8 << 20, transcendentals=0
        ),
        name="project",
    )(me, *heads, *residuals, weight, mixer_gain.reshape(1, width), before_gain.reshape(1, width))


CHUNK = 512
TALL_STEPS = 2


def mix_kernel(units, x, weights, o0, o1, o2, o3, held, hidden, gate_sems, down_sems):
    width = x.shape[1]
    tall = width // TALL_STEPS
    whole = units // CHUNK
    rest = units - whole * CHUNK

    def gate_up(i, start, cols):
        spans = [pl.ds(j * units + start, cols) for j in range(2)]
        return [
            pltpu.make_async_copy(weights.at[:, span], held.at[:, span], gate_sems.at[j, i])
            for j, span in enumerate(spans)
        ]

    def down(i, start):
        rows, cols = pl.ds(start, tall), pl.ds(2 * units, units)
        return pltpu.make_async_copy(weights.at[rows, cols], held.at[rows, cols], down_sems.at[i])

    for i in range(whole):
        for copy in gate_up(i, i * CHUNK, CHUNK):
            copy.start()
    if rest:
        for copy in gate_up(whole, whole * CHUNK, rest):
            copy.start()
    for i in range(TALL_STEPS):
        down(i, i * tall).start()

    def activate(i, start, cols):
        for copy in gate_up(i, start, cols):
            copy.wait()
        gate = jnp.dot(x[...], held[:, pl.ds(start, cols)], preferred_element_type=F32)
        up = jnp.dot(x[...], held[:, pl.ds(units + start, cols)], preferred_element_type=F32)
        hidden[:, pl.ds(start, cols)] = (gate / (1.0 + jnp.exp(-gate)) * up).astype(BF16)

    def gate_step(i, carry):
        activate(i, pl.multiple_of(i * CHUNK, CHUNK), CHUNK)
        return carry

    lax.fori_loop(0, whole, gate_step, 0)
    if rest:
        activate(whole, whole * CHUNK, rest)

    def down_step(i, carry):
        start = pl.multiple_of(i * tall, tall)
        down(i, start).wait()
        part = lax.dot_general(
            hidden[...],
            held[pl.ds(start, tall), 2 * units :],
            (((1,), (1,)), ((), ())),
            preferred_element_type=F32,
        ).astype(BF16)
        for k, out in enumerate((o0, o1, o2, o3)):
            rows = out.shape[0]
            out[:, pl.ds(start, tall)] = part[k * rows : (k + 1) * rows]
        return carry

    lax.fori_loop(0, TALL_STEPS, down_step, 0)


def mix(x, weights, units):
    tokens, width = x.shape
    shape = jax.ShapeDtypeStruct((tokens // 4, width), BF16)
    return pl.pallas_call(
        functools.partial(mix_kernel, units),
        out_shape=(shape,) * 4,
        in_specs=[VMEM, HBM],
        out_specs=(VMEM,) * 4,
        scratch_shapes=[
            pltpu.VMEM(weights.shape, BF16),
            pltpu.VMEM((tokens, units), BF16),
            pltpu.SemaphoreType.DMA((2, pl.cdiv(units, CHUNK))),
            pltpu.SemaphoreType.DMA((TALL_STEPS,)),
        ],
        compiler_params=pltpu.CompilerParams(vmem_limit_bytes=40 << 20),
        cost_estimate=pl.CostEstimate(
            flops=6 * tokens * width * units, bytes_accessed=6 * width * units, transcendentals=0
        ),
        name="mix",
    )(x, weights)


def pack_kernel(gate, up, down, out):
    units = gate.shape[1]
    out[:, :units] = gate[...]
    out[:, units : 2 * units] = up[...]
    out[:, 2 * units :] = down[...]


def pack(gate, up, down):
    return pl.pallas_call(
        pack_kernel,
        out_shape=jax.ShapeDtypeStruct((gate.shape[0], 3 * gate.shape[1]), BF16),
        in_specs=[VMEM] * 3,
        out_specs=VMEM,
        cost_estimate=pl.CostEstimate(flops=1 << 16, bytes_accessed=1 << 19, transcendentals=0),
        name="pack",
    )(gate, up, down.T)


def on_device(
    residual,
    queries,
    key_pairs,
    values,
    lambdas,
    head_gain,
    out_weight,
    mixer_gain,
    before_gain,
    after_gain,
    gate_weight,
    up_weight,
    down_weight,
):
    me = lax.axis_index(T).reshape(1)
    units = gate_weight.shape[1]
    packed = pack(gate_weight, up_weight, down_weight)
    packed, key_pairs, values, queries = lax.optimization_barrier((packed, key_pairs, values, queries))
    weights = lax.all_gather(packed, SP, axis=0, tiled=True)
    kv = jnp.concatenate((key_pairs, values), axis=1)
    beside = [(i, i ^ 1) for i in range(lax.axis_size(X))]
    kv = jnp.concatenate((kv, shifted(kv, X, 2)), axis=0)
    own_queries = jnp.concatenate((queries, lax.ppermute(queries, X, beside)), axis=0)
    queries = (own_queries, shifted(own_queries, C, 1))
    kv, queries = lax.optimization_barrier((kv, queries))
    carried, pieces = None, (kv,)
    above = below = kv
    for step in range(1, lax.axis_size(Z) // 2):
        above, below = shifted(above, Z, 1), shifted(below, Z, -1)
        carried = attend(carried, queries, pieces)
        carried, above, below, residual = lax.optimization_barrier((carried, above, below, residual))
        pieces = (above, below)
        if step == 2:
            residuals = [residual] + [shifted(residual, T, k) for k in (1, 2, 3)]
    half = kv.shape[0] // 2
    far = (shifted(above[:half], Z, 1), shifted(below[half:], Z, -1))
    carried = attend(carried, queries, pieces)
    carried, residuals = lax.optimization_barrier((carried, residuals))
    mine, theirs, _ = attend(carried, queries, far)
    own, sent = join_halves(mine, shifted(theirs, C, 1))
    head_out = merge(lambdas, own, [lax.ppermute(sent, X, beside)], head_gain)

    heads = [head_out] + [shifted(head_out, T, k) for k in (1, 2, 3)]
    normed_in, stream = project(me, heads, residuals, out_weight, mixer_gain, before_gain)
    parts = mix(normed_in, weights, units)
    arrived = [parts[0]] + [shifted(parts[k], T, -k) for k in (2, 1, 3)]
    channel = sum(part.astype(F32) for part in arrived).astype(BF16)
    updated = stream + 0.5 * row_norm(channel.astype(F32), after_gain, 1e-06)
    return updated.astype(BF16)


def solution(mesh):
    finer = Mesh(mesh.devices.reshape(8, 4, 2, mesh.shape[T]), SP_TP)
    in_specs = (
        P(SP_TP, None),
        P(SP, T),
        P(SP, T),
        P(SP, T),
        P(T),
        P(),
        P(),
        P(),
        P(),
        P(),
        P(SP, T),
        P(SP, T),
        P(T, SP),
    )
    return jax.shard_map(
        on_device, mesh=finer, in_specs=in_specs, out_specs=P(SP_TP, None), check_vma=False
    )
```

```python
import functools
import math

import jax
import jax.numpy as jnp
from jax import lax
from jax.experimental import pallas as pl
from jax.experimental.pallas import tpu as pltpu
from jax.sharding import Mesh
from jax.sharding import PartitionSpec as P

HEAD_DIM = 64
WIDTH = 2 * HEAD_DIM
Z, X, C, T = "sp_0", "sp_1", "sp_2", "tp"
SP = (Z, X, C)
SP_TP = (Z, X, C, T)
F32, BF16 = jnp.float32, jnp.bfloat16
LOG2E = 1.4426950408889634
VMEM = pl.BlockSpec(memory_space=pltpu.VMEM)
SMEM = pl.BlockSpec(memory_space=pltpu.SMEM)
HBM = pl.BlockSpec(memory_space=pltpu.HBM)
STATE = WIDTH + 8
COLS = 256
PIECE = 256
TILES = 2
TALL = WIDTH + 16
FACTOR = LOG2E / math.sqrt(HEAD_DIM)
LIMIT = 2.0**80


def shifted(array, axis, by):
    count = lax.axis_size(axis)
    return lax.ppermute(array, axis, [((i + by) % count, i) for i in range(count)])


def attend_kernel(first, count, groups, *refs):
    if first:
        queries, kvs, refs = refs[:2], refs[2 : 2 + count], refs[2 + count :]
        ins, (out_a, out_b, tables, keys2, values1) = None, refs
    else:
        kvs, ins, tables, refs = refs[:count], refs[count : count + 2], refs[count + 2], refs[count + 3 :]
        out_a, out_b, keys2, values1 = refs
    outs = (out_a, out_b)
    length = values1.shape[1]
    lane = lax.broadcasted_iota(jnp.int32, (1, WIDTH), 1)
    values1[WIDTH:, :] = jnp.ones((TALL - WIDTH, length), BF16)
    at = 0
    for kv in kvs:
        span = pl.ds(at, kv.shape[0])
        keys = kv[:, :WIDTH]
        for which in range(2):
            keys2[which, span, :WIDTH] = keys
            keys2[which, span, WIDTH:] = jnp.where((lane < HEAD_DIM) == (which == 0), keys, jnp.ones_like(keys))
        values1[:WIDTH, span] = kv[:, WIDTH:].T
        at += kv.shape[0]
    row = lax.broadcasted_iota(jnp.int32, (WIDTH, COLS), 0)
    if first:

        def one_table(group, carry):
            rows = pl.ds(pl.multiple_of(group * COLS, COLS), COLS)
            for half in range(2):
                for head in range(2):
                    query = queries[half][rows, head * WIDTH : (head + 1) * WIDTH].astype(F32).T * FACTOR
                    high = query.astype(BF16).astype(F32)
                    low = query - high
                    for which in range(2):
                        own = (row < HEAD_DIM) == (which == 0)
                        tile = group * 4 + which * 2 + head
                        table = tables.at[half * 4 * groups + tile]
                        lower = jnp.where(own, low, 0.0)
                        table[:WIDTH, :] = jnp.where(own, high, 0.0).astype(BF16)
                        table[WIDTH:, :] = lower.astype(BF16)
                        score = jnp.dot(keys2[which, :COLS, :], table[...], preferred_element_type=F32)
                        top = jnp.max(score, axis=0, keepdims=True).astype(BF16).astype(F32)
                        spot = HEAD_DIM if which == 0 else 0
                        table[WIDTH:, :] = jnp.where(row == spot, -top, lower).astype(BF16)
                        outs[half][tile, WIDTH:, :] = jnp.broadcast_to(top, (8, COLS))
            return carry

        lax.fori_loop(0, groups, one_table, 0)
    line = lax.broadcasted_iota(jnp.int32, (8, COLS), 0)
    piece = length // pl.cdiv(length, PIECE)

    def stats_of(top, total, reference):
        top, reference = jnp.broadcast_to(top, (8, COLS)), jnp.broadcast_to(reference, (8, COLS))
        return jnp.where(line == 0, top, jnp.where(line == 2, reference, total))

    def one_tile(tile, largest):
        which = lax.rem(tile, 4) // 2
        for half in range(2):
            table = tables[half * 4 * groups + tile]
            both = None
            for start in range(0, length, piece):
                score = jnp.dot(keys2[which, start : start + piece, :], table, preferred_element_type=F32)
                expo = jnp.exp2(score).astype(BF16)
                term = jnp.dot(values1[:, start : start + piece], expo, preferred_element_type=F32)
                both = term if both is None else both + term
            numer, total = both[:WIDTH], both[WIDTH:STATE]
            stats = (outs if first else ins)[half][tile, WIDTH:, :]
            top, reference = stats[0:1], stats[2:3]
            if not first:
                numer = numer + ins[half][tile, :WIDTH, :]
                total = total + stats[1:2]
            outs[half][tile, :WIDTH, :] = numer
            outs[half][tile, WIDTH:, :] = stats_of(top, total, reference)
            fine = (total[0:1] < LIMIT) & (top == reference)
            largest = jnp.maximum(largest, jnp.where(fine, 0.0, 1.0))
        return largest

    def some_tiles(i, largest):
        for j in range(TILES):
            largest = one_tile(i * TILES + j, largest)
        return largest

    largest = lax.fori_loop(0, 4 * groups // TILES, some_tiles, jnp.zeros((1, COLS), F32))

    @pl.when(jnp.max(largest) > 0.0)
    def _():
        def redo_tile(tile, carry):
            which = lax.rem(tile, 4) // 2
            for half in range(2):
                table = tables.at[half * 4 * groups + tile]

                def score_of(i):
                    rows = pl.ds(pl.multiple_of(i * COLS, COLS), COLS)
                    return jnp.dot(keys2[which, rows, :], table[...], preferred_element_type=F32), rows

                def find_top(i, top):
                    return jnp.maximum(top, jnp.max(score_of(i)[0], axis=0, keepdims=True))

                above = lax.fori_loop(0, length // COLS, find_top, jnp.zeros((1, COLS), F32))
                stats = (outs if first else ins)[half][tile, WIDTH:, :]
                old_top, reference = stats[0:1], stats[2:3]
                top = jnp.maximum(old_top, reference + above)
                raised = top - reference

                def add(i, both):
                    score, rows = score_of(i)
                    expo = jnp.exp2(score - raised).astype(BF16)
                    cols = pl.ds(pl.multiple_of(i * COLS, COLS), COLS)
                    return both + jnp.dot(values1[:, cols], expo, preferred_element_type=F32)

                both = lax.fori_loop(0, length // COLS, add, jnp.zeros((TALL, COLS), F32))
                numer, total = both[:WIDTH], both[WIDTH:STATE]
                if not first:
                    shrink = jnp.exp2(old_top - top)
                    numer = numer + ins[half][tile, :WIDTH, :] * shrink
                    total = total + stats[1:2] * shrink
                outs[half][tile, :WIDTH, :] = numer
                outs[half][tile, WIDTH:, :] = stats_of(top, total, reference)
            return carry

        lax.fori_loop(0, 4 * groups, redo_tile, 0)


def attend(carried, queries, kvs):
    first = carried is None
    keys = sum(kv.shape[0] for kv in kvs)
    groups = queries[0].shape[0] // COLS
    state = jax.ShapeDtypeStruct((4 * groups, STATE, COLS), F32)
    tables = jax.ShapeDtypeStruct((8 * groups, 2 * WIDTH, COLS), BF16)
    operands = (*queries, *kvs) if first else (*kvs, *carried)
    results = (state, state, tables) if first else (state, state)
    done = pl.pallas_call(
        functools.partial(attend_kernel, first, len(kvs), groups),
        out_shape=results,
        in_specs=[VMEM] * len(operands),
        out_specs=(VMEM,) * len(results),
        scratch_shapes=[pltpu.VMEM((2, keys, 2 * WIDTH), BF16), pltpu.VMEM((TALL, keys), BF16)],
        compiler_params=pltpu.CompilerParams(vmem_limit_bytes=40 << 20),
        cost_estimate=pl.CostEstimate(
            flops=2 * 2048 * groups * keys * 256 * 2,
            bytes_accessed=keys * 512 + (2 << 20),
            transcendentals=2048 * groups * keys,
        ),
        name="attend",
    )(*operands)
    return done if first else (*done, carried[2])


def joined(mine, theirs, tile):
    a, b = mine[tile, WIDTH:, :], theirs[tile, WIDTH:, :]
    top = jnp.maximum(a[0:1], b[0:1])
    weight_a, weight_b = jnp.exp2(a[0:1] - top), jnp.exp2(b[0:1] - top)
    total = a[1:2] * weight_a + b[1:2] * weight_b
    return weight_a, weight_b, total, top + jnp.log2(total)


def levels_kernel(mine, theirs, out):
    for tile in range(8):
        out[tile : tile + 1, :] = joined(mine, theirs, tile)[3]


def levels_of(mine, theirs):
    return pl.pallas_call(
        levels_kernel,
        out_shape=jax.ShapeDtypeStruct((8, COLS), F32),
        in_specs=[VMEM, VMEM],
        out_specs=VMEM,
        compiler_params=pltpu.CompilerParams(vmem_limit_bytes=8 << 20),
        cost_estimate=pl.CostEstimate(flops=1 << 18, bytes_accessed=1 << 16, transcendentals=0),
        name="levels",
    )(mine, theirs)


def differ_kernel(lambdas, mine, theirs, levels, levels_beside, own, sent):
    for group, out in enumerate((own, sent)):
        for head in range(2):
            shares = []
            for which in range(2):
                kind = which * 2 + head
                tile, same = 4 * group + kind, 4 * (1 - group) + kind
                here, there = levels[tile : tile + 1, :], levels_beside[same : same + 1, :]
                top = jnp.maximum(here, there)
                share = jnp.exp2(here - top) / (jnp.exp2(here - top) + jnp.exp2(there - top))
                weight_a, weight_b, total, _ = joined(mine, theirs, tile)
                share = share / total
                shares.append(mine[tile, :WIDTH, :] * (weight_a * share) + theirs[tile, :WIDTH, :] * (weight_b * share))
            out[head] = (shares[0] - lambdas[head] * shares[1]).astype(out.dtype)


def differ(lambdas, mine, theirs, levels, levels_beside):
    shape = (2, WIDTH, COLS)
    return pl.pallas_call(
        differ_kernel,
        out_shape=(jax.ShapeDtypeStruct(shape, F32), jax.ShapeDtypeStruct(shape, BF16)),
        in_specs=[SMEM] + [VMEM] * 4,
        out_specs=(VMEM, VMEM),
        compiler_params=pltpu.CompilerParams(vmem_limit_bytes=8 << 20),
        cost_estimate=pl.CostEstimate(flops=1 << 22, bytes_accessed=1 << 21, transcendentals=0),
        name="differ",
    )(lambdas, mine, theirs, levels, levels_beside)


def merge_kernel(own, arrived, gain, out):
    for head in range(2):
        attended = own[head] + arrived[head].astype(F32)
        mean_square = jnp.mean(attended * attended, axis=0, keepdims=True)
        normed = attended * lax.rsqrt(mean_square + 1e-05)
        out[:, head * WIDTH : (head + 1) * WIDTH] = (normed.T * gain[...]).astype(BF16)


def merge(own, arrived, gain):
    return pl.pallas_call(
        merge_kernel,
        out_shape=jax.ShapeDtypeStruct((COLS, 2 * WIDTH), BF16),
        in_specs=[VMEM] * 3,
        out_specs=VMEM,
        compiler_params=pltpu.CompilerParams(vmem_limit_bytes=8 << 20),
        cost_estimate=pl.CostEstimate(flops=1 << 22, bytes_accessed=1 << 21, transcendentals=0),
        name="merge",
    )(own, arrived, gain.reshape(1, WIDTH))


def row_norm(rows, gain, epsilon):
    mean_square = jnp.mean(rows * rows, axis=-1, keepdims=True)
    return rows * lax.rsqrt(mean_square + epsilon) * gain


def project_kernel(me, h0, h1, h2, h3, r0, r1, r2, r3, weight, mixer_gain, before_gain, normed_out, stream_out, mixed, held, sems):
    group = h0.shape[1]
    quarter = r0.shape[0]
    copies = []
    for j in range(4):
        rows = pl.ds(pl.multiple_of(lax.rem(me[0] + j, 4) * group, group), group)
        copies.append(pltpu.make_async_copy(weight.at[rows, :], held.at[j], sems.at[j]))
        copies[j].start()
    for j, heads in enumerate((h0, h1, h2, h3)):
        copies[j].wait()
        term = jnp.dot(heads[...], held[j], preferred_element_type=F32)
        if j == 0:
            mixed[...] = term
        else:
            mixed[...] += term
    for k, residual in enumerate((r0, r1, r2, r3)):
        rows = pl.ds(pl.multiple_of(lax.rem(me[0] + k, 4) * quarter, quarter), quarter)
        block = mixed[rows, :].astype(BF16).astype(F32)
        stream = residual[...].astype(F32) + row_norm(block, mixer_gain[...], 1e-06)
        if k == 0:
            stream_out[...] = stream
        normed_out[k * quarter : (k + 1) * quarter, :] = row_norm(stream, before_gain[...], 1e-06).astype(BF16)


def project(me, heads, residuals, weight, mixer_gain, before_gain):
    tokens, width = heads[0].shape[0], weight.shape[1]
    return pl.pallas_call(
        project_kernel,
        out_shape=(
            jax.ShapeDtypeStruct((tokens, width), BF16),
            jax.ShapeDtypeStruct((tokens // 4, width), F32),
        ),
        in_specs=[SMEM] + [VMEM] * 8 + [HBM] + [VMEM] * 2,
        out_specs=(VMEM, VMEM),
        scratch_shapes=[
            pltpu.VMEM((tokens, width), F32),
            pltpu.VMEM((4, weight.shape[0] // 4, width), BF16),
            pltpu.SemaphoreType.DMA((4,)),
        ],
        compiler_params=pltpu.CompilerParams(vmem_limit_bytes=40 << 20),
        cost_estimate=pl.CostEstimate(
            flops=2 * tokens * width * weight.shape[0], bytes_accessed=8 << 20, transcendentals=0
        ),
        name="project",
    )(me, *heads, *residuals, weight, mixer_gain.reshape(1, width), before_gain.reshape(1, width))


CHUNK = 512
TALL_STEPS = 2


def mix_kernel(units, x, weights, o0, o1, o2, o3, held, hidden, gate_sems, down_sems):
    width = x.shape[1]
    tall = width // TALL_STEPS
    whole = units // CHUNK
    rest = units - whole * CHUNK

    def gate_up(i, start, cols):
        spans = [pl.ds(j * units + start, cols) for j in range(2)]
        return [
            pltpu.make_async_copy(weights.at[:, span], held.at[:, span], gate_sems.at[j, i])
            for j, span in enumerate(spans)
        ]

    def down(i, start):
        rows, cols = pl.ds(start, tall), pl.ds(2 * units, units)
        return pltpu.make_async_copy(weights.at[rows, cols], held.at[rows, cols], down_sems.at[i])

    for i in range(whole):
        for copy in gate_up(i, i * CHUNK, CHUNK):
            copy.start()
    if rest:
        for copy in gate_up(whole, whole * CHUNK, rest):
            copy.start()
    for i in range(TALL_STEPS):
        down(i, i * tall).start()

    def activate(i, start, cols):
        for copy in gate_up(i, start, cols):
            copy.wait()
        gate = jnp.dot(x[...], held[:, pl.ds(start, cols)], preferred_element_type=F32)
        up = jnp.dot(x[...], held[:, pl.ds(units + start, cols)], preferred_element_type=F32)
        hidden[:, pl.ds(start, cols)] = (gate / (1.0 + jnp.exp(-gate)) * up).astype(BF16)

    def gate_step(i, carry):
        activate(i, pl.multiple_of(i * CHUNK, CHUNK), CHUNK)
        return carry

    lax.fori_loop(0, whole, gate_step, 0)
    if rest:
        activate(whole, whole * CHUNK, rest)

    def down_step(i, carry):
        start = pl.multiple_of(i * tall, tall)
        down(i, start).wait()
        part = lax.dot_general(
            hidden[...],
            held[pl.ds(start, tall), 2 * units :],
            (((1,), (1,)), ((), ())),
            preferred_element_type=F32,
        ).astype(BF16)
        for k, out in enumerate((o0, o1, o2, o3)):
            rows = out.shape[0]
            out[:, pl.ds(start, tall)] = part[k * rows : (k + 1) * rows]
        return carry

    lax.fori_loop(0, TALL_STEPS, down_step, 0)


def mix(x, weights, units):
    tokens, width = x.shape
    shape = jax.ShapeDtypeStruct((tokens // 4, width), BF16)
    return pl.pallas_call(
        functools.partial(mix_kernel, units),
        out_shape=(shape,) * 4,
        in_specs=[VMEM, HBM],
        out_specs=(VMEM,) * 4,
        scratch_shapes=[
            pltpu.VMEM(weights.shape, BF16),
            pltpu.VMEM((tokens, units), BF16),
            pltpu.SemaphoreType.DMA((2, pl.cdiv(units, CHUNK))),
            pltpu.SemaphoreType.DMA((TALL_STEPS,)),
        ],
        compiler_params=pltpu.CompilerParams(vmem_limit_bytes=40 << 20),
        cost_estimate=pl.CostEstimate(
            flops=6 * tokens * width * units, bytes_accessed=6 * width * units, transcendentals=0
        ),
        name="mix",
    )(x, weights)


def pack_kernel(gate, up, down, out):
    units = gate.shape[1]
    out[:, :units] = gate[...]
    out[:, units : 2 * units] = up[...]
    out[:, 2 * units :] = down[...]


def pack(gate, up, down):
    return pl.pallas_call(
        pack_kernel,
        out_shape=jax.ShapeDtypeStruct((gate.shape[0], 3 * gate.shape[1]), BF16),
        in_specs=[VMEM] * 3,
        out_specs=VMEM,
        cost_estimate=pl.CostEstimate(flops=1 << 16, bytes_accessed=1 << 19, transcendentals=0),
        name="pack",
    )(gate, up, down.T)


def on_device(
    residual,
    queries,
    key_pairs,
    values,
    lambdas,
    head_gain,
    out_weight,
    mixer_gain,
    before_gain,
    after_gain,
    gate_weight,
    up_weight,
    down_weight,
):
    me = lax.axis_index(T).reshape(1)
    units = gate_weight.shape[1]
    packed = pack(gate_weight, up_weight, down_weight)
    packed, key_pairs, values, queries = lax.optimization_barrier((packed, key_pairs, values, queries))
    weights = lax.all_gather(packed, SP, axis=0, tiled=True)
    kv = jnp.concatenate((key_pairs, values), axis=1)
    beside = [(i, i ^ 1) for i in range(lax.axis_size(X))]
    kv = jnp.concatenate((kv, shifted(kv, X, 2)), axis=0)
    own_queries = jnp.concatenate((queries, lax.ppermute(queries, X, beside)), axis=0)
    queries = (own_queries, shifted(own_queries, C, 1))
    kv, queries = lax.optimization_barrier((kv, queries))
    carried, pieces = None, (kv,)
    above = below = kv
    for step in range(1, lax.axis_size(Z) // 2):
        above, below = shifted(above, Z, 1), shifted(below, Z, -1)
        carried = attend(carried, queries, pieces)
        carried, above, below, residual = lax.optimization_barrier((carried, above, below, residual))
        pieces = (above, below)
        if step == 2:
            residuals = [residual] + [shifted(residual, T, k) for k in (1, 2, 3)]
    half = kv.shape[0] // 2
    far = (shifted(above[:half], Z, 1), shifted(below[half:], Z, -1))
    carried = attend(carried, queries, pieces)
    carried, residuals = lax.optimization_barrier((carried, residuals))
    mine, theirs, _ = attend(carried, queries, far)
    theirs = shifted(theirs, C, 1)
    levels = levels_of(mine, theirs)
    own, sent = differ(lambdas, mine, theirs, levels, lax.ppermute(levels, X, beside))
    head_out = merge(own, lax.ppermute(sent, X, beside), head_gain)

    heads = [head_out] + [shifted(head_out, T, k) for k in (1, 2, 3)]
    normed_in, stream = project(me, heads, residuals, out_weight, mixer_gain, before_gain)
    parts = mix(normed_in, weights, units)
    arrived = [parts[0]] + [shifted(parts[k], T, -k) for k in (2, 1, 3)]
    channel = sum(part.astype(F32) for part in arrived).astype(BF16)
    updated = stream + 0.5 * row_norm(channel.astype(F32), after_gain, 1e-06)
    return updated.astype(BF16)


def solution(mesh):
    finer = Mesh(mesh.devices.reshape(8, 4, 2, mesh.shape[T]), SP_TP)
    in_specs = (
        P(SP_TP, None),
        P(SP, T),
        P(SP, T),
        P(SP, T),
        P(T),
        P(),
        P(),
        P(),
        P(),
        P(),
        P(SP, T),
        P(SP, T),
        P(T, SP),
    )
    return jax.shard_map(
        on_device, mesh=finer, in_specs=in_specs, out_specs=P(SP_TP, None), check_vma=False
    )
```

```python
import functools
import math

import jax
import jax.numpy as jnp
from jax import lax
from jax.experimental import pallas as pl
from jax.experimental.pallas import tpu as pltpu
from jax.sharding import Mesh
from jax.sharding import PartitionSpec as P

HEAD_DIM = 64
WIDTH = 2 * HEAD_DIM
Z, X, C, T = "sp_0", "sp_1", "sp_2", "tp"
SP = (Z, X, C)
SP_TP = (Z, X, C, T)
F32, BF16 = jnp.float32, jnp.bfloat16
LOG2E = 1.4426950408889634
VMEM = pl.BlockSpec(memory_space=pltpu.VMEM)
SMEM = pl.BlockSpec(memory_space=pltpu.SMEM)
HBM = pl.BlockSpec(memory_space=pltpu.HBM)
STATE = WIDTH + 8
COLS = 256
PIECE = 256
TILES = 2
TALL = WIDTH + 16
FACTOR = LOG2E / math.sqrt(HEAD_DIM)
LIMIT = 2.0**80


def shifted(array, axis, by):
    count = lax.axis_size(axis)
    return lax.ppermute(array, axis, [((i + by) % count, i) for i in range(count)])


def attend_kernel(first, count, groups, *refs):
    if first:
        queries, kvs, refs = refs[:2], refs[2 : 2 + count], refs[2 + count :]
        ins, (out_a, out_b, tables, keys2, values1) = None, refs
    else:
        kvs, ins, tables, refs = refs[:count], refs[count : count + 2], refs[count + 2], refs[count + 3 :]
        out_a, out_b, keys2, values1 = refs
    outs = (out_a, out_b)
    length = values1.shape[1]
    lane = lax.broadcasted_iota(jnp.int32, (1, WIDTH), 1)
    values1[WIDTH:, :] = jnp.ones((TALL - WIDTH, length), BF16)
    at = 0
    for kv in kvs:
        span = pl.ds(at, kv.shape[0])
        keys = kv[:, :WIDTH]
        for which in range(2):
            keys2[which, span, :WIDTH] = keys
            keys2[which, span, WIDTH:] = jnp.where((lane < HEAD_DIM) == (which == 0), keys, jnp.ones_like(keys))
        values1[:WIDTH, span] = kv[:, WIDTH:].T
        at += kv.shape[0]
    row = lax.broadcasted_iota(jnp.int32, (WIDTH, COLS), 0)
    if first:

        def one_table(group, carry):
            rows = pl.ds(pl.multiple_of(group * COLS, COLS), COLS)
            for half in range(2):
                for head in range(2):
                    query = queries[half][rows, head * WIDTH : (head + 1) * WIDTH].astype(F32).T * FACTOR
                    high = query.astype(BF16).astype(F32)
                    low = query - high
                    for which in range(2):
                        own = (row < HEAD_DIM) == (which == 0)
                        tile = group * 4 + which * 2 + head
                        table = tables.at[half * 4 * groups + tile]
                        lower = jnp.where(own, low, 0.0)
                        table[:WIDTH, :] = jnp.where(own, high, 0.0).astype(BF16)
                        table[WIDTH:, :] = lower.astype(BF16)
                        score = jnp.dot(keys2[which, :COLS, :], table[...], preferred_element_type=F32)
                        top = jnp.max(score, axis=0, keepdims=True).astype(BF16).astype(F32)
                        spot = HEAD_DIM if which == 0 else 0
                        table[WIDTH:, :] = jnp.where(row == spot, -top, lower).astype(BF16)
                        outs[half][tile, WIDTH:, :] = jnp.broadcast_to(top, (8, COLS))
            return carry

        lax.fori_loop(0, groups, one_table, 0)
    line = lax.broadcasted_iota(jnp.int32, (8, COLS), 0)
    piece = length // pl.cdiv(length, PIECE)

    def stats_of(top, total, reference):
        top, reference = jnp.broadcast_to(top, (8, COLS)), jnp.broadcast_to(reference, (8, COLS))
        return jnp.where(line == 0, top, jnp.where(line == 2, reference, total))

    def one_tile(tile, largest):
        which = lax.rem(tile, 4) // 2
        for half in range(2):
            table = tables[half * 4 * groups + tile]
            both = None
            for start in range(0, length, piece):
                score = jnp.dot(keys2[which, start : start + piece, :], table, preferred_element_type=F32)
                expo = jnp.exp2(score).astype(BF16)
                term = jnp.dot(values1[:, start : start + piece], expo, preferred_element_type=F32)
                both = term if both is None else both + term
            numer, total = both[:WIDTH], both[WIDTH:STATE]
            stats = (outs if first else ins)[half][tile, WIDTH:, :]
            top, reference = stats[0:1], stats[2:3]
            if not first:
                numer = numer + ins[half][tile, :WIDTH, :]
                total = total + stats[1:2]
            outs[half][tile, :WIDTH, :] = numer
            outs[half][tile, WIDTH:, :] = stats_of(top, total, reference)
            fine = (total[0:1] < LIMIT) & (top == reference)
            largest = jnp.maximum(largest, jnp.where(fine, 0.0, 1.0))
        return largest

    def some_tiles(i, largest):
        for j in range(TILES):
            largest = one_tile(i * TILES + j, largest)
        return largest

    largest = lax.fori_loop(0, 4 * groups // TILES, some_tiles, jnp.zeros((1, COLS), F32))

    @pl.when(jnp.max(largest) > 0.0)
    def _():
        def redo_tile(tile, carry):
            which = lax.rem(tile, 4) // 2
            for half in range(2):
                table = tables.at[half * 4 * groups + tile]

                def score_of(i):
                    rows = pl.ds(pl.multiple_of(i * COLS, COLS), COLS)
                    return jnp.dot(keys2[which, rows, :], table[...], preferred_element_type=F32), rows

                def find_top(i, top):
                    return jnp.maximum(top, jnp.max(score_of(i)[0], axis=0, keepdims=True))

                above = lax.fori_loop(0, length // COLS, find_top, jnp.zeros((1, COLS), F32))
                stats = (outs if first else ins)[half][tile, WIDTH:, :]
                old_top, reference = stats[0:1], stats[2:3]
                top = jnp.maximum(old_top, reference + above)
                raised = top - reference

                def add(i, both):
                    score, rows = score_of(i)
                    expo = jnp.exp2(score - raised).astype(BF16)
                    cols = pl.ds(pl.multiple_of(i * COLS, COLS), COLS)
                    return both + jnp.dot(values1[:, cols], expo, preferred_element_type=F32)

                both = lax.fori_loop(0, length // COLS, add, jnp.zeros((TALL, COLS), F32))
                numer, total = both[:WIDTH], both[WIDTH:STATE]
                if not first:
                    shrink = jnp.exp2(old_top - top)
                    numer = numer + ins[half][tile, :WIDTH, :] * shrink
                    total = total + stats[1:2] * shrink
                outs[half][tile, :WIDTH, :] = numer
                outs[half][tile, WIDTH:, :] = stats_of(top, total, reference)
            return carry

        lax.fori_loop(0, 4 * groups, redo_tile, 0)


def attend(carried, queries, kvs):
    first = carried is None
    keys = sum(kv.shape[0] for kv in kvs)
    groups = queries[0].shape[0] // COLS
    state = jax.ShapeDtypeStruct((4 * groups, STATE, COLS), F32)
    tables = jax.ShapeDtypeStruct((8 * groups, 2 * WIDTH, COLS), BF16)
    operands = (*queries, *kvs) if first else (*kvs, *carried)
    results = (state, state, tables) if first else (state, state)
    done = pl.pallas_call(
        functools.partial(attend_kernel, first, len(kvs), groups),
        out_shape=results,
        in_specs=[VMEM] * len(operands),
        out_specs=(VMEM,) * len(results),
        scratch_shapes=[pltpu.VMEM((2, keys, 2 * WIDTH), BF16), pltpu.VMEM((TALL, keys), BF16)],
        compiler_params=pltpu.CompilerParams(vmem_limit_bytes=40 << 20),
        cost_estimate=pl.CostEstimate(
            flops=2 * 2048 * groups * keys * 256 * 2,
            bytes_accessed=keys * 512 + (2 << 20),
            transcendentals=2048 * groups * keys,
        ),
        name="attend",
    )(*operands)
    return done if first else (*done, carried[2])


def joined(mine, theirs, tile):
    a, b = mine[tile, WIDTH:, :], theirs[tile, WIDTH:, :]
    top = jnp.maximum(a[0:1], b[0:1])
    weight_a, weight_b = jnp.exp2(a[0:1] - top), jnp.exp2(b[0:1] - top)
    total = a[1:2] * weight_a + b[1:2] * weight_b
    return weight_a, weight_b, total, top + jnp.log2(total)


def levels_kernel(mine, theirs, out):
    for tile in range(8):
        out[tile : tile + 1, :] = joined(mine, theirs, tile)[3]


def levels_of(mine, theirs):
    return pl.pallas_call(
        levels_kernel,
        out_shape=jax.ShapeDtypeStruct((8, COLS), F32),
        in_specs=[VMEM, VMEM],
        out_specs=VMEM,
        compiler_params=pltpu.CompilerParams(vmem_limit_bytes=8 << 20),
        cost_estimate=pl.CostEstimate(flops=1 << 18, bytes_accessed=1 << 16, transcendentals=0),
        name="levels",
    )(mine, theirs)


def differ_kernel(lambdas, mine, theirs, levels, levels_beside, own, sent):
    for group, out in enumerate((own, sent)):
        for head in range(2):
            shares = []
            for which in range(2):
                kind = which * 2 + head
                tile, same = 4 * group + kind, 4 * (1 - group) + kind
                here, there = levels[tile : tile + 1, :], levels_beside[same : same + 1, :]
                top = jnp.maximum(here, there)
                share = jnp.exp2(here - top) / (jnp.exp2(here - top) + jnp.exp2(there - top))
                weight_a, weight_b, total, _ = joined(mine, theirs, tile)
                share = share / total
                shares.append(mine[tile, :WIDTH, :] * (weight_a * share) + theirs[tile, :WIDTH, :] * (weight_b * share))
            out[head] = (shares[0] - lambdas[head] * shares[1]).astype(out.dtype)


def differ(lambdas, mine, theirs, levels, levels_beside):
    shape = (2, WIDTH, COLS)
    return pl.pallas_call(
        differ_kernel,
        out_shape=(jax.ShapeDtypeStruct(shape, F32), jax.ShapeDtypeStruct(shape, BF16)),
        in_specs=[SMEM] + [VMEM] * 4,
        out_specs=(VMEM, VMEM),
        compiler_params=pltpu.CompilerParams(vmem_limit_bytes=8 << 20),
        cost_estimate=pl.CostEstimate(flops=1 << 22, bytes_accessed=1 << 21, transcendentals=0),
        name="differ",
    )(lambdas, mine, theirs, levels, levels_beside)


def merge_kernel(own, arrived, gain, out):
    for head in range(2):
        attended = own[head] + arrived[head].astype(F32)
        mean_square = jnp.mean(attended * attended, axis=0, keepdims=True)
        normed = attended * lax.rsqrt(mean_square + 1e-05)
        out[:, head * WIDTH : (head + 1) * WIDTH] = (normed.T * gain[...]).astype(BF16)


def merge(own, arrived, gain):
    return pl.pallas_call(
        merge_kernel,
        out_shape=jax.ShapeDtypeStruct((COLS, 2 * WIDTH), BF16),
        in_specs=[VMEM] * 3,
        out_specs=VMEM,
        compiler_params=pltpu.CompilerParams(vmem_limit_bytes=8 << 20),
        cost_estimate=pl.CostEstimate(flops=1 << 22, bytes_accessed=1 << 21, transcendentals=0),
        name="merge",
    )(own, arrived, gain.reshape(1, WIDTH))


def row_norm(rows, gain, epsilon):
    mean_square = jnp.mean(rows * rows, axis=-1, keepdims=True)
    return rows * lax.rsqrt(mean_square + epsilon) * gain


def project_kernel(me, h0, h1, h2, h3, r0, r1, r2, r3, weight, mixer_gain, before_gain, normed_out, stream_out, mixed, held, sems):
    group = h0.shape[1]
    quarter = r0.shape[0]
    copies = []
    for j in range(4):
        rows = pl.ds(pl.multiple_of(lax.rem(me[0] + j, 4) * group, group), group)
        copies.append(pltpu.make_async_copy(weight.at[rows, :], held.at[j], sems.at[j]))
        copies[j].start()
    for j, heads in enumerate((h0, h1, h2, h3)):
        copies[j].wait()
        term = jnp.dot(heads[...], held[j], preferred_element_type=F32)
        if j == 0:
            mixed[...] = term
        else:
            mixed[...] += term
    for k, residual in enumerate((r0, r1, r2, r3)):
        rows = pl.ds(pl.multiple_of(lax.rem(me[0] + k, 4) * quarter, quarter), quarter)
        block = mixed[rows, :].astype(BF16).astype(F32)
        stream = residual[...].astype(F32) + row_norm(block, mixer_gain[...], 1e-06)
        if k == 0:
            stream_out[...] = stream
        normed_out[k * quarter : (k + 1) * quarter, :] = row_norm(stream, before_gain[...], 1e-06).astype(BF16)


def project(me, heads, residuals, weight, mixer_gain, before_gain):
    tokens, width = heads[0].shape[0], weight.shape[1]
    return pl.pallas_call(
        project_kernel,
        out_shape=(
            jax.ShapeDtypeStruct((tokens, width), BF16),
            jax.ShapeDtypeStruct((tokens // 4, width), F32),
        ),
        in_specs=[SMEM] + [VMEM] * 8 + [HBM] + [VMEM] * 2,
        out_specs=(VMEM, VMEM),
        scratch_shapes=[
            pltpu.VMEM((tokens, width), F32),
            pltpu.VMEM((4, weight.shape[0] // 4, width), BF16),
            pltpu.SemaphoreType.DMA((4,)),
        ],
        compiler_params=pltpu.CompilerParams(vmem_limit_bytes=40 << 20),
        cost_estimate=pl.CostEstimate(
            flops=2 * tokens * width * weight.shape[0], bytes_accessed=8 << 20, transcendentals=0
        ),
        name="project",
    )(me, *heads, *residuals, weight, mixer_gain.reshape(1, width), before_gain.reshape(1, width))


CHUNK = 512
TALL_STEPS = 2


def mix_kernel(units, x, weights, o0, o1, o2, o3, held, hidden, gate_sems, down_sems):
    width = x.shape[1]
    tall = width // TALL_STEPS
    whole = units // CHUNK
    rest = units - whole * CHUNK

    def gate_up(i, start, cols):
        spans = [pl.ds(j * units + start, cols) for j in range(2)]
        return [
            pltpu.make_async_copy(weights.at[:, span], held.at[:, span], gate_sems.at[j, i])
            for j, span in enumerate(spans)
        ]

    def down(i, start):
        rows, cols = pl.ds(start, tall), pl.ds(2 * units, units)
        return pltpu.make_async_copy(weights.at[rows, cols], held.at[rows, cols], down_sems.at[i])

    for i in range(whole):
        for copy in gate_up(i, i * CHUNK, CHUNK):
            copy.start()
    if rest:
        for copy in gate_up(whole, whole * CHUNK, rest):
            copy.start()
    for i in range(TALL_STEPS):
        down(i, i * tall).start()

    def activate(i, start, cols):
        for copy in gate_up(i, start, cols):
            copy.wait()
        gate = jnp.dot(x[...], held[:, pl.ds(start, cols)], preferred_element_type=F32)
        up = jnp.dot(x[...], held[:, pl.ds(units + start, cols)], preferred_element_type=F32)
        hidden[:, pl.ds(start, cols)] = (gate / (1.0 + jnp.exp(-gate)) * up).astype(BF16)

    def gate_step(i, carry):
        activate(i, pl.multiple_of(i * CHUNK, CHUNK), CHUNK)
        return carry

    lax.fori_loop(0, whole, gate_step, 0)
    if rest:
        activate(whole, whole * CHUNK, rest)

    def down_step(i, carry):
        start = pl.multiple_of(i * tall, tall)
        down(i, start).wait()
        part = lax.dot_general(
            hidden[...],
            held[pl.ds(start, tall), 2 * units :],
            (((1,), (1,)), ((), ())),
            preferred_element_type=F32,
        ).astype(BF16)
        for k, out in enumerate((o0, o1, o2, o3)):
            rows = out.shape[0]
            out[:, pl.ds(start, tall)] = part[k * rows : (k + 1) * rows]
        return carry

    lax.fori_loop(0, TALL_STEPS, down_step, 0)


def mix(x, weights, units):
    tokens, width = x.shape
    shape = jax.ShapeDtypeStruct((tokens // 4, width), BF16)
    return pl.pallas_call(
        functools.partial(mix_kernel, units),
        out_shape=(shape,) * 4,
        in_specs=[VMEM, HBM],
        out_specs=(VMEM,) * 4,
        scratch_shapes=[
            pltpu.VMEM(weights.shape, BF16),
            pltpu.VMEM((tokens, units), BF16),
            pltpu.SemaphoreType.DMA((2, pl.cdiv(units, CHUNK))),
            pltpu.SemaphoreType.DMA((TALL_STEPS,)),
        ],
        compiler_params=pltpu.CompilerParams(vmem_limit_bytes=40 << 20),
        cost_estimate=pl.CostEstimate(
            flops=6 * tokens * width * units, bytes_accessed=6 * width * units, transcendentals=0
        ),
        name="mix",
    )(x, weights)


def pack_kernel(gate, up, down, out):
    units = gate.shape[1]
    out[:, :units] = gate[...]
    out[:, units : 2 * units] = up[...]
    out[:, 2 * units :] = down[...]


def pack(gate, up, down):
    return pl.pallas_call(
        pack_kernel,
        out_shape=jax.ShapeDtypeStruct((gate.shape[0], 3 * gate.shape[1]), BF16),
        in_specs=[VMEM] * 3,
        out_specs=VMEM,
        cost_estimate=pl.CostEstimate(flops=1 << 16, bytes_accessed=1 << 19, transcendentals=0),
        name="pack",
    )(gate, up, down.T)


def on_device(
    residual,
    queries,
    key_pairs,
    values,
    lambdas,
    head_gain,
    out_weight,
    mixer_gain,
    before_gain,
    after_gain,
    gate_weight,
    up_weight,
    down_weight,
):
    me = lax.axis_index(T).reshape(1)
    units = gate_weight.shape[1]
    packed = pack(gate_weight, up_weight, down_weight)
    packed, key_pairs, values, queries = lax.optimization_barrier((packed, key_pairs, values, queries))
    weights = lax.all_gather(packed, SP, axis=0, tiled=True)
    kv = jnp.concatenate((key_pairs, values), axis=1)
    beside = [(i, i ^ 1) for i in range(lax.axis_size(X))]
    kv = jnp.concatenate((kv, shifted(kv, X, 2)), axis=0)
    own_queries = jnp.concatenate((queries, lax.ppermute(queries, X, beside)), axis=0)
    queries = (own_queries, shifted(own_queries, C, 1))
    kv, queries = lax.optimization_barrier((kv, queries))
    carried, pieces = None, (kv,)
    above = below = kv
    for step in range(1, lax.axis_size(Z) // 2):
        above, below = shifted(above, Z, 1), shifted(below, Z, -1)
        carried = attend(carried, queries, pieces)
        carried, above, below, residual = lax.optimization_barrier((carried, above, below, residual))
        pieces = (above, below)
        if step == 2:
            residuals = [residual] + [shifted(residual, T, k) for k in (1, 2, 3)]
    half = kv.shape[0] // 2
    far = (shifted(above[:half], Z, 1), shifted(below[half:], Z, -1))
    carried = attend(carried, queries, pieces)
    carried, residuals = lax.optimization_barrier((carried, residuals))
    mine, theirs, _ = attend(carried, queries, far)
    theirs = shifted(theirs, C, 1)
    levels = levels_of(mine, theirs)
    own, sent = differ(lambdas, mine, theirs, levels, lax.ppermute(levels, X, beside))
    head_out = merge(own, lax.ppermute(sent, X, beside), head_gain)

    heads = [head_out] + [shifted(head_out, T, k) for k in (1, 2, 3)]
    normed_in, stream = project(me, heads, residuals, out_weight, mixer_gain, before_gain)
    parts = mix(normed_in, weights, units)
    arrived = [parts[0]] + [shifted(parts[k], T, -k) for k in (1, 3, 2)]
    channel = sum(part.astype(F32) for part in arrived).astype(BF16)
    updated = stream + 0.5 * row_norm(channel.astype(F32), after_gain, 1e-06)
    return updated.astype(BF16)


def solution(mesh):
    finer = Mesh(mesh.devices.reshape(8, 4, 2, mesh.shape[T]), SP_TP)
    in_specs = (
        P(SP_TP, None),
        P(SP, T),
        P(SP, T),
        P(SP, T),
        P(T),
        P(),
        P(),
        P(),
        P(),
        P(),
        P(SP, T),
        P(SP, T),
        P(T, SP),
    )
    return jax.shard_map(
        on_device, mesh=finer, in_specs=in_specs, out_specs=P(SP_TP, None), check_vma=False
    )
```
